128 devices in a mesh: sp: 64 (over z, y, x), tp: 2 (over core).
Axes of the slice: x: 4, y: 4, z: 4, core: 2. Of those that a mesh axis runs over, the one named last changes fastest.
Arguments:
- query_small: bfloat16 [24576, 2, 128], P('sp', 'tp'), may hold values from -8 to 8
- key_small: bfloat16 [24576, 2, 128], P('sp', 'tp'), may hold values from -8 to 8
- value_small: bfloat16 [24576, 2, 128], P('sp', 'tp'), may hold values from -6 to 6
- query_large: bfloat16 [24576, 2, 256], P('sp', 'tp'), may hold values from -8 to 8
- key_large: bfloat16 [24576, 2, 256], P('sp', 'tp'), may hold values from -8 to 8
- value_large: bfloat16 [24576, 2, 128], P('sp', 'tp'), may hold values from -6 to 6
- lambdas: float32 [2, 2], P('tp'), may hold values from 0.3 to 0.8
- slopes: float32 [2, 2], P('tp'), as said below
- head_gain: bfloat16 [128], replicated, may hold values from 0.099609375 to 1.8984375
- residual: bfloat16 [24576, 2048], P(('sp', 'tp')), may hold values from -6 to 6
- out_weight: bfloat16 [512, 2048], replicated, may hold values from -0.25 to 0.25
- norm_gains: bfloat16 [2, 2048], replicated, may hold values from 0.099609375 to 1.8984375
- routes: int32 [24576, 2], P(('sp', 'tp')), may hold values from 0 to 63, as said below
- route_weights: float32 [24576, 2], P(('sp', 'tp')), may hold values from 0.1 to 1
- gate_weight: bfloat16 [64, 2048, 1024], P('sp', None, 'tp'), may hold values from -0.125 to 0.125
- up_weight: bfloat16 [64, 2048, 1024], P('sp', None, 'tp'), may hold values from -0.125 to 0.125
- down_weight: bfloat16 [64, 1024, 2048], P('sp', 'tp'), may hold values from -0.1875 to 0.1875
Outputs:
- layer_out: bfloat16 [24576, 2048], P(('sp', 'tp'))
The draws below stay inside these ranges and needn't reach their ends.
Inputs may be any that keep to these rules, and one draw needn't show every extreme that they name: `slopes`: positive. `routes`: each token names two different experts of one group of 16 consecutive expert numbers. In each aligned block of 192 rows (the tokens of one device) no expert is named more than 12 times, and some expert is named exactly 12 times in every block.
All inputs are finite; a program needn't handle non-finite values.
Results may differ from the reference program's by a relative error of at most 0.011.
Values may be sent and summed in bfloat16 or wider, within the bound.
No kernel may reach another device: no remote copies, remote signals or barrier semaphores. Data moves between devices by JAX's collectives and lax.ppermute only.
A program may use at most 128 MiB of HBM per device.

```python
import math
import jax
import jax.numpy as jnp
from jax import lax

D = 2048
HG = 2
DS = 64
DL = 128
DV = 128
FF = 1024
TOPK = 2
GROUPS = 4
TOKENS = 24576
ROWS = 192
EXPERTS = 64
CAP = 12
N_TP = 2


def paired_draw(key, key_width):
    folded = jax.random.fold_in(key, 1000 + key_width)
    query_key, keyset_key = jax.random.split(folded, 2)
    spread = math.sqrt(1.75)
    queries = jnp.clip(jax.random.normal(query_key, (TOKENS, HG, 2 * key_width), jnp.float32) * spread, -8.0, 8.0)
    keyset = jnp.clip(jax.random.normal(keyset_key, (TOKENS, HG, 2 * key_width), jnp.float32) * spread, -8.0, 8.0)
    return (queries, keyset)


def draw_query_small(key, part):
    return paired_draw(key, DS)[0].astype(jnp.bfloat16)


def draw_key_small(key, part):
    return paired_draw(key, DS)[1].astype(jnp.bfloat16)


def draw_query_large(key, part):
    return paired_draw(key, DL)[0].astype(jnp.bfloat16)


def draw_key_large(key, part):
    return paired_draw(key, DL)[1].astype(jnp.bfloat16)


def draw_slopes(key, part):
    folded = jax.random.fold_in(key, 7)
    order_key, level_key = jax.random.split(folded)
    ranking = jax.random.permutation(order_key, 2 * HG)
    levels = jax.random.uniform(level_key, (2 * HG,), jnp.float32)
    slower = jnp.exp(math.log(0.25 / TOKENS) + levels * math.log(8.0))
    faster = jnp.exp(math.log(1.0 / 16.0) + levels * math.log(2.0))
    keeping = HG
    return jnp.where(ranking < keeping, slower, faster).reshape(HG, 2).astype(jnp.float32)


def draw_routes(key, part):
    folded = jax.random.fold_in(key, 11)
    group_key, blocks_key = jax.random.split(folded)
    group_size = EXPERTS // GROUPS
    halfway = ROWS // 2
    busiest = jax.random.randint(group_key, (), 0, GROUPS)

    def one_block(block_key):
        first_key, second_key, offset_key, permute_key, swap_key, order_key = jax.random.split(block_key, 6)
        first_cut = jax.random.randint(first_key, (), 0, halfway + 1)
        second_cut = jax.random.randint(second_key, (), 0, halfway + 1)
        lower_cut = jnp.minimum(first_cut, second_cut)
        upper_cut = jnp.maximum(first_cut, second_cut)
        others = (busiest + 1 + jnp.arange(GROUPS - 1)) % GROUPS
        counts = jnp.zeros((GROUPS,), jnp.int32).at[busiest].set(halfway)
        counts = counts.at[others].set(jnp.stack([lower_cut, upper_cut - lower_cut, halfway - upper_cut]).astype(jnp.int32))
        group_ends = jnp.cumsum(counts)
        starts = group_ends - counts
        position = jnp.arange(ROWS)
        chosen = jnp.sum((position[:, None] >= group_ends[None, :]).astype(jnp.int32), axis=1)
        within = position - starts[chosen]
        offsets = jax.random.randint(offset_key, (GROUPS,), 1, group_size)
        permuted = jax.vmap(lambda sub_key: jax.random.permutation(sub_key, group_size))(jax.random.split(permute_key, GROUPS))
        leading = permuted[chosen, within % group_size]
        trailing = permuted[chosen, (within + offsets[chosen]) % group_size]
        pair_ids = jnp.stack([leading, trailing], axis=1) + (chosen * group_size)[:, None]
        swapped = jax.random.randint(swap_key, (ROWS,), 0, 2)
        pair_ids = jnp.where(swapped[:, None] == 1, pair_ids[:, ::-1], pair_ids)
        shuffle = jax.random.permutation(order_key, ROWS)
        return pair_ids[shuffle]
    block_keys = jax.random.split(blocks_key, TOKENS // ROWS)
    return jax.vmap(one_block)(block_keys).reshape(TOKENS, 2).astype(jnp.int32)


def shard_levels(rng, dims, shards, low, top_value):
    gain, own = 1.0, jax.random.fold_in(rng, 6)
    for dim, blocks in shards:
        draws = jnp.exp(jax.random.uniform(jax.random.fold_in(own, dim), (blocks,), jnp.float32, low / len(shards), top_value / len(shards)))
        gain = gain * jnp.repeat(draws, dims[dim] // blocks).reshape([-1 if axis == dim else 1 for axis in range(len(dims))])
    return gain


def normal_values(key, shape, scale, most, cuts=(), held_as=jnp.bfloat16):
    values = scale * jax.random.normal(key, shape, jnp.float32)
    if cuts:
        values = values * shard_levels(key, shape, cuts, -0.22, 0.18)
    return jnp.clip(values, -most, most).astype(held_as)


def setup_inputs(seed: int = 0) -> dict:
    arg_keys = jax.random.split(jax.random.key(seed), 18)
    return {
        "query_small": draw_query_small(jax.random.fold_in(arg_keys[17], 71), 0),
        "key_small": draw_key_small(jax.random.fold_in(arg_keys[17], 71), 0),
        "value_small": normal_values(arg_keys[2], (TOKENS, HG, DV), 1.0, 6.0, ((0, 64), (1, 2))),
        "query_large": draw_query_large(jax.random.fold_in(arg_keys[17], 71), 0),
        "key_large": draw_key_large(jax.random.fold_in(arg_keys[17], 71), 0),
        "value_large": normal_values(arg_keys[5], (TOKENS, HG, DV), 1.0, 6.0, ((0, 64), (1, 2))),
        "lambdas": jnp.clip(0.3 + 0.5 * jax.random.uniform(arg_keys[6], (HG, 2), jnp.float32) ** shard_levels(arg_keys[6], (HG, 2), ((0, 2),), -0.2, 0.2), 0.3, 0.8),
        "slopes": draw_slopes(jax.random.fold_in(arg_keys[17], 71), 0),
        "head_gain": jnp.clip(1.0 + 0.18 * jax.random.normal(arg_keys[8], (DV,), jnp.float32), 0.099609375, 1.8984375).astype(jnp.bfloat16),
        "residual": normal_values(arg_keys[9], (TOKENS, D), 1.0, 6.0, ((0, 128),)),
        "out_weight": normal_values(arg_keys[10], (2 * HG * DV, D), (2 * HG * DV) ** -0.5, 0.25),
        "norm_gains": jnp.clip(1.0 + 0.18 * jax.random.normal(arg_keys[11], (2, D), jnp.float32), 0.099609375, 1.8984375).astype(jnp.bfloat16),
        "routes": draw_routes(jax.random.fold_in(arg_keys[17], 71), 0),
        "route_weights": jnp.clip(0.1 + 0.9 * jax.random.uniform(arg_keys[13], (TOKENS, TOPK), jnp.float32) ** shard_levels(arg_keys[13], (TOKENS, TOPK), ((0, 128),), -0.2, 0.2), 0.1, 1.0),
        "gate_weight": normal_values(arg_keys[14], (EXPERTS, D, FF), D ** -0.5, 0.125, ((0, 64), (2, 2))),
        "up_weight": normal_values(arg_keys[15], (EXPERTS, D, FF), D ** -0.5, 0.125, ((0, 64), (2, 2))),
        "down_weight": normal_values(arg_keys[16], (EXPERTS, FF, D), FF ** -0.5, 0.1875, ((0, 64), (1, 2))),
    }


residual_gain = 8.0 ** 0.25
epsilon = 1e-05

def layer_norm(values, gain_row):
    average = lax.optimization_barrier(jnp.mean(values, axis=-1, keepdims=True))
    centred = values - average
    variance = lax.optimization_barrier(jnp.mean(centred * centred, axis=-1, keepdims=True))
    return centred * lax.rsqrt(variance + epsilon) * gain_row.astype(jnp.float32)

def group_attention(queries, keyset, valueset, lambda_row, slope_row, head_gain):
    length, head_count, doubled = queries.shape
    key_width = doubled // 2
    query_four = queries.reshape(length, head_count, 2, key_width).astype(jnp.float32)
    key_four = keyset.reshape(length, head_count, 2, key_width).astype(jnp.float32)
    value_all = valueset.astype(jnp.float32)
    block_rows = math.gcd(length, 512)
    key_places = jnp.arange(length, dtype=jnp.int32)

    def one_block(number):
        query_block = lax.dynamic_slice_in_dim(query_four, number * block_rows, block_rows, 0)
        query_places = number * block_rows + jnp.arange(block_rows, dtype=jnp.int32)
        distance = (query_places[:, None] - key_places[None, :]).astype(jnp.float32)
        scores = jnp.einsum('qhmd,khmd->hmqk', query_block, key_four) * key_width ** (-0.5)
        scores = scores - slope_row[:, None, None, None] * distance
        scores = jnp.where(distance >= 0, scores, -jnp.inf)
        highest = lax.optimization_barrier(jnp.max(scores, axis=-1, keepdims=True))
        exponent = jnp.exp(scores - highest)
        totals = lax.optimization_barrier(jnp.sum(exponent, axis=-1))
        rounded = lax.optimization_barrier(exponent.astype(jnp.bfloat16)).astype(jnp.float32)
        mixture = jnp.einsum('hmqk,khe->hmqe', rounded, value_all) / totals[..., None]
        head_out = mixture[:, 0] - lambda_row[:, None, None] * mixture[:, 1]
        scaled = head_out * lax.rsqrt(lax.optimization_barrier(jnp.mean(head_out * head_out, axis=-1, keepdims=True)) + epsilon)
        scaled = scaled * head_gain.astype(jnp.float32)
        return jnp.transpose(scaled, (1, 0, 2))
    blocks = lax.map(one_block, jnp.arange(length // block_rows, dtype=jnp.int32))
    return blocks.reshape(length, head_count, -1)

def expert_pass(middle, routes, route_weights, gate_weight, up_weight, down_weight):
    pair_ids = routes.reshape(-1).astype(jnp.int32)
    pair_count = pair_ids.shape[0]
    ordering = jnp.argsort(pair_ids, stable=True).astype(jnp.int32)
    counts = lax.optimization_barrier(jnp.sum((pair_ids[None, :] == jnp.arange(EXPERTS, dtype=jnp.int32)[:, None]).astype(jnp.int32), axis=1))
    starts = (jnp.cumsum(counts) - counts).astype(jnp.int32)
    most_rows = CAP * (TOKENS // ROWS)
    padded = jnp.concatenate([ordering, jnp.zeros((most_rows,), jnp.int32)])
    part_width = FF // N_TP
    features = middle.shape[1]

    def per_expert(collected, expert):
        slot_rows = lax.dynamic_slice_in_dim(padded, starts[expert], most_rows, 0)
        in_use = jnp.arange(most_rows, dtype=jnp.int32) < counts[expert]
        inputs = middle[slot_rows // 2]
        gate_in = jnp.dot(inputs, gate_weight[expert], preferred_element_type=jnp.float32)
        up_in = jnp.dot(inputs, up_weight[expert], preferred_element_type=jnp.float32)
        hidden = (jax.nn.silu(gate_in) * up_in).astype(jnp.bfloat16)
        summed = jnp.zeros((most_rows, features), jnp.float32)
        for number in range(N_TP):
            partial_value = jnp.dot(hidden[:, number * part_width:(number + 1) * part_width], down_weight[expert, number * part_width:(number + 1) * part_width], preferred_element_type=jnp.float32)
            summed = summed + lax.optimization_barrier(partial_value.astype(jnp.bfloat16)).astype(jnp.float32)
        result = lax.optimization_barrier(summed.astype(jnp.bfloat16)).astype(jnp.float32)
        collected = collected.at[slot_rows].add(jnp.where(in_use[:, None], result, 0.0))
        return (collected, None)
    pair_out, _ = lax.scan(per_expert, jnp.zeros((pair_count, features), jnp.float32), jnp.arange(EXPERTS, dtype=jnp.int32))
    weighted = route_weights.reshape(-1, 1) * pair_out
    return lax.optimization_barrier(jnp.sum(weighted.reshape(TOKENS, TOPK, features), axis=1))

def reference(query_small, key_small, value_small, query_large, key_large, value_large, lambdas, slopes, head_gain, residual, out_weight, norm_gains, routes, route_weights, gate_weight, up_weight, down_weight):
    small_out = group_attention(query_small, key_small, value_small, lambdas[:, 0], slopes[:, 0], head_gain)
    large_out = group_attention(query_large, key_large, value_large, lambdas[:, 1], slopes[:, 1], head_gain)
    attended = jnp.stack([small_out, large_out], axis=2).astype(jnp.bfloat16).reshape(TOKENS, -1)
    projected = jnp.dot(attended, out_weight, preferred_element_type=jnp.float32)
    middle = layer_norm(residual_gain * residual.astype(jnp.float32) + projected, norm_gains[0]).astype(jnp.bfloat16)
    moe_sum = expert_pass(middle, routes, route_weights, gate_weight, up_weight, down_weight)
    return layer_norm(residual_gain * middle.astype(jnp.float32) + moe_sum, norm_gains[1]).astype(jnp.bfloat16)
```

```python
import math

import jax
import jax.numpy as jnp
from jax import lax
from jax.experimental import pallas as pl
from jax.experimental.pallas import tpu as pltpu
from jax.sharding import Mesh, PartitionSpec as P

residual_gain = 8.0**0.25
epsilon = 1e-05
masked_score = -1e30

LOG2E = 1.4426950408889634


def flash_body(meta, slope, qt, keys, values, out, lse, qs, bias, top, acc, *, chunk, place_count, span, lanes):
    block = pl.program_id(0)
    plane = meta[0]
    place = meta[1]
    width = qt.shape[1]
    half = width // 2
    scale = LOG2E * half ** (-0.5)
    slope_two = slope[0] * LOG2E
    rows = span * chunk
    total = 2 * chunk
    qs[...] = jnp.zeros_like(qs)
    qs[:half, :chunk] = qt[0, :half, :]
    qs[half:, chunk:] = qt[0, half:, :]
    bias[...] = slope_two * lax.broadcasted_iota(jnp.int32, bias.shape, 0).astype(jnp.float32)
    top[...] = jnp.full_like(top, masked_score)
    acc[...] = jnp.zeros_like(acc)
    last_query = (block - plane) * (place_count * chunk) + place * chunk + (chunk - 1)

    def step(number, masked):
        shift = slope_two * (number * rows - last_query).astype(jnp.float32)
        key_block = keys[pl.ds(pl.multiple_of(number * rows, rows), rows), :]
        value_parts = [values[number * span + i] for i in range(span)]
        value_block = jnp.concatenate(value_parts, axis=1) if span > 1 else value_parts[0]
        value_block = jnp.concatenate([value_block, jnp.ones((16, rows), jnp.bfloat16)], axis=0)
        for first in range(0, total, lanes):
            cut = slice(first, first + lanes)
            scores = jnp.dot(key_block, qs[:, cut], preferred_element_type=jnp.float32)
            scores = scores * scale + bias[...]
            if masked:
                lane = lax.broadcasted_iota(jnp.int32, (rows, lanes), 1) + first
                lane = jnp.where(lane >= chunk, lane - chunk, lane)
                key_place = lax.broadcasted_iota(jnp.int32, (rows, lanes), 0) + number * rows
                scores = jnp.where(key_place <= lane + place * chunk, scores, masked_score)
            old = top[:, cut]
            new = jnp.maximum(old, jnp.max(scores, axis=0, keepdims=True) + shift)
            probs = jnp.exp2(scores - (new - shift)).astype(jnp.bfloat16)
            product = jnp.dot(value_block, probs, preferred_element_type=jnp.float32)
            acc[:, cut] = acc[:, cut] * jnp.exp2(old - new) + product
            top[:, cut] = new

    full = jnp.where(block > plane, place_count // span, jnp.where(block == plane, place // span, 0))

    def loop(number, carry):
        step(number, False)
        return carry

    lax.fori_loop(0, full, loop, 0)

    @pl.when(block == plane)
    def _():
        step(place // span, True)

    vsize = acc.shape[0] - 16
    sums = jnp.maximum(acc[vsize : vsize + 1, :], 1e-30)
    mixed = acc[:vsize, :] * (1.0 / sums)
    out[0, :, :vsize] = mixed[:, :chunk].T.astype(jnp.bfloat16)
    out[0, :, vsize:] = mixed[:, chunk:].T.astype(jnp.bfloat16)
    lse[0] = top[...] + jnp.log2(sums)


def flash(meta, slope, qt, keys, values, span=2, lanes=256):
    blocks, width, chunk = qt.shape
    place_count, vsize, _ = values.shape
    rows = span * chunk
    body = lambda *refs: flash_body(*refs, chunk=chunk, place_count=place_count, span=span, lanes=lanes)
    return pl.pallas_call(
        body,
        grid=(blocks,),
        in_specs=[
            pl.BlockSpec(memory_space=pltpu.SMEM),
            pl.BlockSpec(memory_space=pltpu.SMEM),
            pl.BlockSpec((1, width, chunk), lambda b: (b, 0, 0)),
            pl.BlockSpec((place_count * chunk, width), lambda b: (0, 0)),
            pl.BlockSpec((place_count, vsize, chunk), lambda b: (0, 0, 0)),
        ],
        out_specs=[
            pl.BlockSpec((1, chunk, 2 * vsize), lambda b: (b, 0, 0)),
            pl.BlockSpec((1, 1, 2 * chunk), lambda b: (b, 0, 0)),
        ],
        out_shape=[
            jax.ShapeDtypeStruct((blocks, chunk, 2 * vsize), jnp.bfloat16),
            jax.ShapeDtypeStruct((blocks, 1, 2 * chunk), jnp.float32),
        ],
        scratch_shapes=[
            pltpu.VMEM((width, 2 * chunk), jnp.bfloat16),
            pltpu.VMEM((rows, lanes), jnp.float32),
            pltpu.VMEM((1, 2 * chunk), jnp.float32),
            pltpu.VMEM((vsize + 16, 2 * chunk), jnp.float32),
        ],
        compiler_params=pltpu.CompilerParams(
            dimension_semantics=("arbitrary",), vmem_limit_bytes=56 * 1024 * 1024
        ),
    )(meta, slope, qt, keys, values)


def cut_along(shard, dim, size):
    before, after = (shard.shape[:dim], shard.shape[dim + 1 :])
    return jnp.moveaxis(shard.reshape(*before, size, -1, *after), dim, 0)


def sent_and_summed(shard, axis, dim):
    blocks = cut_along(shard, dim, lax.axis_size(axis))
    arrived = lax.all_to_all(blocks, axis, split_axis=0, concat_axis=0, tiled=True)
    return arrived.astype(jnp.float32).sum(axis=0)


def layer_norm(values, gain_row):
    average = jnp.mean(values, axis=-1, keepdims=True)
    centred = values - average
    variance = jnp.mean(centred * centred, axis=-1, keepdims=True)
    return centred * lax.rsqrt(variance + epsilon) * gain_row.astype(jnp.float32)


SP = ("z", "y", "x")
PLANE = ("y", "x")
OWNERS = ("z", "tp")


def exchanged(part_out, part_lse, core_count, value_size):
    planes, length, _ = part_out.shape
    row_count = length // core_count
    sent = part_out.reshape(planes * core_count, row_count, -1)
    arrived = lax.all_to_all(sent, OWNERS, split_axis=0, concat_axis=0, tiled=True)
    levels = part_lse.reshape(planes, 2, core_count, row_count)
    levels = jnp.transpose(levels, (0, 2, 1, 3)).reshape(planes * core_count, 2, row_count)
    levels = lax.all_to_all(levels, OWNERS, split_axis=0, concat_axis=0, tiled=True)
    levels = levels.reshape(planes, core_count, 2, row_count)
    weights = jnp.exp2(levels - jnp.max(levels, axis=0, keepdims=True))
    weights = weights / jnp.sum(weights, axis=0, keepdims=True)
    parts = arrived.reshape(planes, core_count, row_count, 2, value_size).astype(jnp.float32)
    weights = jnp.transpose(weights, (0, 1, 3, 2))[..., None]
    return jnp.sum(weights * parts, axis=0)


def finish(mixture, lambda_column, head_gain):
    head_out = mixture[:, :, 0] - lambda_column[:, None, None] * mixture[:, :, 1]
    scaled = head_out * lax.rsqrt(jnp.mean(head_out * head_out, axis=-1, keepdims=True) + epsilon)
    return scaled * head_gain.astype(jnp.float32)


def shards(
    query_small,
    key_small,
    value_small,
    query_large,
    key_large,
    value_large,
    lambdas,
    slopes,
    head_gain,
    residual,
    out_weight,
    norm_gains,
    routes,
    route_weights,
    gate_weight,
    up_weight,
    down_weight,
):
    length = query_small.shape[0]
    planes = lax.axis_size("z")
    places = lax.axis_size("y") * lax.axis_size("x")
    value_size = value_small.shape[2]
    plane = lax.axis_index("z")
    place = lax.axis_index(PLANE)
    mirror = [(i, planes - 1 - i) for i in range(planes)]
    large_pack = jnp.concatenate([key_large.reshape(length, -1), value_large.reshape(length, -1)], axis=1)
    large_pack = lax.ppermute(large_pack, "z", mirror)
    key_width = key_large.shape[2]
    small_keys = lax.all_gather(key_small.reshape(length, -1), PLANE, axis=0, tiled=True)
    small_values = lax.all_gather(value_small.reshape(length, -1).T, PLANE, axis=0)
    small_queries = lax.all_gather(query_small.reshape(length, -1).T, "z", axis=0)
    large_queries = lax.all_gather(query_large.reshape(length, -1).T, "z", axis=0)
    large_keys = lax.all_gather(large_pack[:, :key_width], PLANE, axis=0, tiled=True)
    large_values = lax.all_gather(large_pack[:, key_width:].T, PLANE, axis=0)
    small_meta = jnp.stack([plane, place]).astype(jnp.int32)
    large_meta = jnp.stack([planes - 1 - plane, place]).astype(jnp.int32)
    small_out, small_lse = flash(small_meta, slopes[0, :1], small_queries, small_keys, small_values)
    large_out, large_lse = flash(large_meta, slopes[0, 1:], large_queries, large_keys, large_values)
    core_count = lax.axis_size("tp")
    row_count = length // core_count
    small_mixed = exchanged(small_out, small_lse, core_count, value_size)
    large_mixed = exchanged(large_out, large_lse, core_count, value_size)
    all_lambdas = lax.all_gather(lambdas[0], "tp", axis=0)
    attended = jnp.stack(
        [
            finish(small_mixed, all_lambdas[:, 0], head_gain),
            finish(large_mixed, all_lambdas[:, 1], head_gain),
        ],
        axis=1,
    ).astype(jnp.bfloat16)
    regrouped = jnp.transpose(attended, (2, 0, 1, 3)).reshape(row_count, -1)
    projected = jnp.dot(regrouped, out_weight, preferred_element_type=jnp.float32)
    middle = layer_norm(
        residual_gain * residual.astype(jnp.float32) + projected, norm_gains[0]
    ).astype(jnp.bfloat16)
    experts = lax.axis_size(SP)
    capacity = 4 * row_count // experts
    features = middle.shape[1]
    chosen = routes.reshape(-1)
    matches = (chosen[:, None] == jnp.arange(experts)[None, :]).astype(jnp.int32)
    earlier = jnp.cumsum(matches, axis=0) - matches
    target = chosen * capacity + jnp.sum(earlier * matches, axis=1)
    selector = jnp.any(
        target.reshape(row_count, 2)[None, :, :] == jnp.arange(experts * capacity)[:, None, None],
        axis=2,
    ).astype(jnp.bfloat16)
    outgoing = jnp.dot(selector, middle, preferred_element_type=jnp.float32).astype(jnp.bfloat16)
    outgoing = outgoing.reshape(experts, capacity, features)
    arrived = lax.all_to_all(outgoing, SP, split_axis=0, concat_axis=0, tiled=True)
    paired = lax.all_gather(arrived, "tp", axis=0, tiled=True).reshape(-1, features)
    gate_in = jnp.dot(paired, gate_weight[0], preferred_element_type=jnp.float32)
    upward = jnp.dot(paired, up_weight[0], preferred_element_type=jnp.float32)
    hidden = (jax.nn.silu(gate_in) * upward).astype(jnp.bfloat16)
    partial_value = jnp.dot(hidden, down_weight[0], preferred_element_type=jnp.float32).astype(
        jnp.bfloat16
    )
    summed = sent_and_summed(
        lax.optimization_barrier(partial_value).astype(jnp.float32).astype(jnp.bfloat16), "tp", 0
    ).astype(jnp.bfloat16)
    returned = lax.all_to_all(
        summed.reshape(experts, capacity, features), SP, split_axis=0, concat_axis=0, tiled=True
    )
    expert_out = returned.reshape(experts * capacity, features)
    picked = jnp.take(expert_out, target, axis=0).reshape(row_count, 2, features)
    moe_sum = jnp.sum(route_weights[:, :, None] * picked.astype(jnp.float32), axis=1)
    return layer_norm(residual_gain * middle.astype(jnp.float32) + moe_sum, norm_gains[1]).astype(
        jnp.bfloat16
    )


def solution(mesh):
    cube = Mesh(mesh.devices.reshape(4, 4, 4, 2), ("z", "y", "x", "tp"))
    both = SP + ("tp",)
    placed = (
        P(SP, "tp", None),
        P(SP, "tp", None),
        P(SP, "tp", None),
        P(SP, "tp", None),
        P(SP, "tp", None),
        P(SP, "tp", None),
        P("tp", None),
        P("tp", None),
        P(),
        P(both, None),
        P(),
        P(),
        P(both, None),
        P(both, None),
        P(SP, None, "tp"),
        P(SP, None, "tp"),
        P(SP, "tp", None),
    )
    return jax.shard_map(
        shards, mesh=cube, in_specs=placed, out_specs=P(both, None), check_vma=False
    )
```

```python
import jax
import jax.numpy as jnp
from jax import lax
from jax.experimental import pallas as pl
from jax.experimental.pallas import tpu as pltpu
from jax.sharding import Mesh, PartitionSpec as P

residual_gain = 8.0**0.25
epsilon = 1e-05
masked_score = -1e30
LOG2E = 1.4426950408889634
SP = ("z", "y", "x")
PLANE = ("y", "x")
OWNERS = ("z", "tp")
SPAN = 2
LANES = 256
VMEM_LIMIT = 56 * 1024 * 1024


def three_parts(value):
    high = value.astype(jnp.bfloat16).astype(jnp.float32)
    rest = value - high
    middle = rest.astype(jnp.bfloat16).astype(jnp.float32)
    return high, middle, (rest - middle).astype(jnp.bfloat16).astype(jnp.float32)


def flash_group(plane, place, slope, qt, keys, values, qs, bias, top, acc, sbuf, mbuf):
    block = pl.program_id(0)
    place_count, chunk, width = keys.shape
    half = width // 2
    scale = LOG2E * half ** (-0.5)
    slope_two = slope * LOG2E
    rows = SPAN * chunk
    total = 2 * chunk
    qs[:width, :] = jnp.zeros((width, total), jnp.bfloat16)
    qs[:half, :chunk] = qt[0, :half, :]
    qs[half:width, chunk:] = qt[0, half:, :]
    bias[...] = slope_two * lax.broadcasted_iota(jnp.int32, bias.shape, 0).astype(jnp.float32)
    top[...] = jnp.full_like(top, masked_score)
    acc[...] = jnp.zeros_like(acc)
    last_query = (block - plane) * (place_count * chunk) + place * chunk + (chunk - 1)
    cuts = [slice(first, first + LANES) for first in range(0, total, LANES)]

    def fill(number, slot):
        key_block = keys[pl.ds(number * SPAN, SPAN)].reshape(rows, width)
        for cut in cuts:
            scores = jnp.dot(key_block, qs[:width, cut], preferred_element_type=jnp.float32)
            scores = scores * scale + bias[...]
            sbuf[slot, :, cut] = scores
            mbuf[slot, :, cut] = jnp.max(scores, axis=0, keepdims=True)

    def use(number, slot):
        shift = slope_two * (number * rows - last_query).astype(jnp.float32)
        value_block = jnp.concatenate([values[number * SPAN + i] for i in range(SPAN)], axis=1)
        value_block = jnp.concatenate([value_block, jnp.ones((16, rows), jnp.bfloat16)], axis=0)
        for cut in cuts:
            old = top[:, cut]
            new = jnp.maximum(old, mbuf[slot, :, cut] + shift)
            probs = jnp.exp2(sbuf[slot, :, cut] - (new - shift)).astype(jnp.bfloat16)
            top[:, cut] = new
            product = jnp.dot(value_block, probs, preferred_element_type=jnp.float32)
            acc[:, cut] = acc[:, cut] * jnp.exp2(old - new) + product

    def hide_later_keys(number, slot):
        for cut in cuts:
            lane = lax.broadcasted_iota(jnp.int32, (rows, LANES), 1) + cut.start
            lane = jnp.where(lane >= chunk, lane - chunk, lane)
            key_place = lax.broadcasted_iota(jnp.int32, (rows, LANES), 0) + number * rows
            scores = jnp.where(key_place <= lane + place * chunk, sbuf[slot, :, cut], masked_score)
            sbuf[slot, :, cut] = scores
            mbuf[slot, :, cut] = jnp.max(scores, axis=0, keepdims=True)

    most = place_count // SPAN
    count = jnp.where(block > plane, most, jnp.where(block == plane, place // SPAN + 1, 0))

    @pl.when(count > 0)
    def _():
        fill(0, 0)
        last = count - 1

        def pair_step(pair, carry):
            fill(2 * pair + 1, 1)
            use(2 * pair, 0)
            fill(jnp.minimum(2 * pair + 2, most - 1), 0)
            use(2 * pair + 1, 1)
            return carry

        lax.fori_loop(0, last // 2, pair_step, 0)

        @pl.when(last % 2 == 1)
        def _():
            fill(last, 1)
            use(last - 1, 0)

            @pl.when(block == plane)
            def _():
                hide_later_keys(last, 1)

            use(last, 1)

        @pl.when(last % 2 == 0)
        def _():
            @pl.when(block == plane)
            def _():
                hide_later_keys(last, 0)

            use(last, 0)


def flash_body(
    meta, slopes, lambdas, small_q, large_q, small_k, large_k, small_v, large_v,
    out, qs, bias, top, acc, sbuf, mbuf, tail,
):
    chunk = small_q.shape[2]
    vsize = small_v.shape[1]
    tail[...] = jnp.zeros_like(tail)
    groups = (
        (meta[0], small_q, small_k, small_v),
        (meta[2], large_q, large_k, large_v),
    )
    for number, (plane, qt, keys, values) in enumerate(groups):
        flash_group(
            plane, meta[1], slopes[number], qt, keys, values, qs, bias, top, acc, sbuf, mbuf
        )
        sums = jnp.maximum(acc[vsize : vsize + 1, :], 1e-30)
        mixed = acc[:vsize, :] * (1.0 / sums)
        level = top[...] + jnp.log2(sums)
        lam = jnp.full((1, chunk), lambdas[number], jnp.float32)
        for j in range(2):
            column = (2 * number + j) * vsize
            out[0, :, column : column + vsize] = (
                mixed[:, j * chunk : (j + 1) * chunk].T.astype(jnp.bfloat16)
            )
            for k, part in enumerate(three_parts(level[:, j * chunk : (j + 1) * chunk])):
                row = 6 * k + 2 * number + j
                tail[row : row + 1, :] = part
        for k, part in enumerate(three_parts(lam)):
            row = 6 * k + 4 + number
            tail[row : row + 1, :] = part
    out[0, :, 4 * vsize :] = tail[...].T.astype(jnp.bfloat16)


def flash(meta, slopes, lambdas, small_q, large_q, gathered):
    blocks, small_width, chunk = small_q.shape
    large_width = large_q.shape[1]
    place_count, _, _ = gathered.shape
    vsize = 128
    rows = SPAN * chunk
    scalar = pl.BlockSpec(memory_space=pltpu.SMEM)
    return pl.pallas_call(
        flash_body,
        grid=(blocks,),
        in_specs=[
            scalar,
            scalar,
            scalar,
            pl.BlockSpec((1, small_width, chunk), lambda b: (b, 0, 0)),
            pl.BlockSpec((1, large_width, chunk), lambda b: (b, 0, 0)),
            pl.BlockSpec((place_count, chunk, small_width), lambda b: (0, 0, 2)),
            pl.BlockSpec((place_count, chunk, large_width), lambda b: (0, 0, 0)),
            pl.BlockSpec((place_count, vsize, chunk), lambda b: (0, 3, 0)),
            pl.BlockSpec((place_count, vsize, chunk), lambda b: (0, 4, 0)),
        ],
        out_specs=pl.BlockSpec((1, chunk, 5 * vsize), lambda b: (b, 0, 0)),
        out_shape=jax.ShapeDtypeStruct((blocks, chunk, 5 * vsize), jnp.bfloat16),
        scratch_shapes=[
            pltpu.VMEM((large_width, 2 * chunk), jnp.bfloat16),
            pltpu.VMEM((rows, LANES), jnp.float32),
            pltpu.VMEM((1, 2 * chunk), jnp.float32),
            pltpu.VMEM((vsize + 16, 2 * chunk), jnp.float32),
            pltpu.VMEM((2, rows, 2 * chunk), jnp.float32),
            pltpu.VMEM((2, 1, 2 * chunk), jnp.float32),
            pltpu.VMEM((vsize, chunk), jnp.float32),
        ],
        compiler_params=pltpu.CompilerParams(
            dimension_semantics=("arbitrary",), vmem_limit_bytes=VMEM_LIMIT
        ),
    )(meta, slopes, lambdas, small_q, large_q, gathered, gathered, gathered, gathered)


def normed(values, gain_row):
    average = jnp.mean(values, axis=-1, keepdims=True)
    centred = values - average
    variance = jnp.mean(centred * centred, axis=-1, keepdims=True)
    return centred * lax.rsqrt(variance + epsilon) * gain_row


def merge_body(core, arrived, head_gain, residual, weight, norm_gain, middle, keep, give):
    planes = arrived.shape[0] // 2
    vsize = head_gain.shape[1]
    gain = head_gain[...].astype(jnp.float32)
    pieces = []
    for head in range(2):
        tails = []
        for z in range(planes):
            lanes = arrived[2 * z + head, :, 4 * vsize :].astype(jnp.float32)
            tails.append([lanes[:, i : i + 1] + lanes[:, i + 6 : i + 7] + lanes[:, i + 12 : i + 13] for i in range(6)])
        for group in range(2):
            mixtures = []
            for j in range(2):
                index = 2 * group + j
                highest = tails[0][index]
                for z in range(1, planes):
                    highest = jnp.maximum(highest, tails[z][index])
                weights = [jnp.exp2(tails[z][index] - highest) for z in range(planes)]
                scaled = 1.0 / sum(weights)
                column = index * vsize
                mixtures.append(
                    sum(
                        (weights[z] * scaled)
                        * arrived[2 * z + head, :, column : column + vsize].astype(jnp.float32)
                        for z in range(planes)
                    )
                )
            head_out = mixtures[0] - tails[0][4 + group] * mixtures[1]
            power = jnp.mean(head_out * head_out, axis=-1, keepdims=True)
            pieces.append((head_out * lax.rsqrt(power + epsilon) * gain).astype(jnp.bfloat16))
    attended = jnp.concatenate(pieces, axis=1)
    projected = jnp.dot(attended, weight[...], preferred_element_type=jnp.float32)
    values = residual_gain * residual[...].astype(jnp.float32) + projected
    result = normed(values, norm_gain[...].astype(jnp.float32)).astype(jnp.bfloat16)
    middle[...] = result
    half = result.shape[1] // 2

    @pl.when(core[0] == 0)
    def _():
        keep[...] = result[:, :half]
        give[...] = result[:, half:]

    @pl.when(core[0] == 1)
    def _():
        keep[...] = result[:, half:]
        give[...] = result[:, :half]


def merge(core, arrived, head_gain, residual, weight, norm_gain):
    count, features = residual.shape
    return pl.pallas_call(
        merge_body,
        in_specs=[pl.BlockSpec(memory_space=pltpu.SMEM)] + [pl.BlockSpec(memory_space=pltpu.VMEM)] * 5,
        out_shape=[
            jax.ShapeDtypeStruct((count, features), jnp.bfloat16),
            jax.ShapeDtypeStruct((count, features // 2), jnp.bfloat16),
            jax.ShapeDtypeStruct((count, features // 2), jnp.bfloat16),
        ],
        compiler_params=pltpu.CompilerParams(vmem_limit_bytes=VMEM_LIMIT),
    )(core, arrived, head_gain, residual, weight, norm_gain)


def expert_body(core, mine, other, gate, up, down, keep, give):
    half = mine.shape[1]
    first = pl.multiple_of(core[0] * half, half)
    second = pl.multiple_of((1 - core[0]) * half, half)
    own_rows = mine[...]
    other_rows = other[...]

    def through(weight):
        return jnp.dot(
            own_rows, weight[0, pl.ds(first, half), :], preferred_element_type=jnp.float32
        ) + jnp.dot(
            other_rows, weight[0, pl.ds(second, half), :], preferred_element_type=jnp.float32
        )

    gate_in = through(gate)
    upward = through(up)
    hidden = (gate_in * (1.0 / (1.0 + jnp.exp(-gate_in))) * upward).astype(jnp.bfloat16)
    keep[...] = jnp.dot(
        hidden, down[0, :, pl.ds(first, half)], preferred_element_type=jnp.float32
    ).astype(jnp.bfloat16)
    give[...] = jnp.dot(
        hidden, down[0, :, pl.ds(second, half)], preferred_element_type=jnp.float32
    ).astype(jnp.bfloat16)


def expert(core, mine, other, gate, up, down):
    count, half = mine.shape
    block_rows = 256
    rows = pl.BlockSpec((block_rows, half), lambda i: (i, 0))
    shape = jax.ShapeDtypeStruct((count, half), jnp.bfloat16)
    return pl.pallas_call(
        expert_body,
        grid=(count // block_rows,),
        in_specs=[
            pl.BlockSpec(memory_space=pltpu.SMEM),
            rows,
            rows,
            pl.BlockSpec(gate.shape, lambda i: (0, 0, 0)),
            pl.BlockSpec(up.shape, lambda i: (0, 0, 0)),
            pl.BlockSpec(down.shape, lambda i: (0, 0, 0)),
        ],
        out_specs=[rows, rows],
        out_shape=[shape, shape],
        compiler_params=pltpu.CompilerParams(
            dimension_semantics=("arbitrary",), vmem_limit_bytes=VMEM_LIMIT
        ),
    )(core, mine, other, gate, up, down)


def final_body(core, own, received, middle, norm_gain, out, total):
    half = own.shape[1]

    @pl.when(core[0] == 0)
    def _():
        total[:, :half] = own[...]
        total[:, half:] = received[...]

    @pl.when(core[0] == 1)
    def _():
        total[:, :half] = received[...]
        total[:, half:] = own[...]

    values = residual_gain * middle[...].astype(jnp.float32) + total[...]
    out[...] = normed(values, norm_gain[...].astype(jnp.float32)).astype(jnp.bfloat16)


def final(core, own, received, middle, norm_gain):
    return pl.pallas_call(
        final_body,
        in_specs=[pl.BlockSpec(memory_space=pltpu.SMEM)] + [pl.BlockSpec(memory_space=pltpu.VMEM)] * 4,
        out_shape=jax.ShapeDtypeStruct(middle.shape, jnp.bfloat16),
        scratch_shapes=[pltpu.VMEM(middle.shape, jnp.float32)],
        compiler_params=pltpu.CompilerParams(vmem_limit_bytes=VMEM_LIMIT),
    )(core, own, received, middle, norm_gain)


def slots(routes, experts, block, offset):
    chosen = routes.reshape(-1)
    matches = (chosen[:, None] == jnp.arange(experts)[None, :]).astype(jnp.int32)
    earlier = jnp.cumsum(matches, axis=0) - matches
    rank = jnp.sum(earlier * matches, axis=1)
    return (chosen * block + offset + rank).reshape(routes.shape)


def shards(
    query_small,
    key_small,
    value_small,
    query_large,
    key_large,
    value_large,
    lambdas,
    slopes,
    head_gain,
    residual,
    out_weight,
    norm_gains,
    routes,
    route_weights,
    gate_weight,
    up_weight,
    down_weight,
):
    length = query_small.shape[0]
    planes = lax.axis_size("z")
    plane = lax.axis_index("z")
    place = lax.axis_index(PLANE)
    core = lax.axis_index("tp")
    mirror = [(i, planes - 1 - i) for i in range(planes)]
    swap = [(0, 1), (1, 0)]
    key_width = key_large.shape[2]
    large_pack = jnp.concatenate(
        [key_large.reshape(length, -1), value_large.reshape(length, -1)], axis=1
    )
    large_pack = lax.ppermute(large_pack, "z", mirror)
    packed = jnp.concatenate(
        [
            jnp.concatenate([large_pack[:, :key_width], key_small.reshape(length, -1)], axis=1),
            value_small.reshape(length, -1).T,
            large_pack[:, key_width:].T,
        ],
        axis=0,
    )
    gathered = lax.all_gather(packed, PLANE, axis=0)
    small_queries = lax.all_gather(query_small.reshape(length, -1).T, "z", axis=0)
    large_queries = lax.all_gather(query_large.reshape(length, -1).T, "z", axis=0)

    core_count = lax.axis_size("tp")
    row_count = length // core_count
    experts = lax.axis_size(SP)
    block = core_count * (4 * row_count // experts)
    their_routes = lax.ppermute(routes, "tp", swap)
    their_weights = lax.ppermute(route_weights, "tp", swap)
    capacity = block // core_count
    target = jnp.concatenate(
        [
            slots(routes, experts, block, core * capacity),
            slots(their_routes, experts, block, (1 - core) * capacity),
        ],
        axis=0,
    )
    shares = jnp.concatenate([route_weights, their_weights], axis=0)
    places = jnp.arange(experts * block)
    hits = [target[:, k] for k in range(2)]
    selector = (
        (hits[0][None, :] == places[:, None]) | (hits[1][None, :] == places[:, None])
    ).astype(jnp.bfloat16)
    spread = jnp.where(hits[0][:, None] == places[None, :], shares[:, :1], 0.0) + jnp.where(
        hits[1][:, None] == places[None, :], shares[:, 1:], 0.0
    )
    spread_top = lax.reduce_precision(spread, exponent_bits=8, mantissa_bits=7)
    spread_high = spread_top.astype(jnp.bfloat16)
    spread_low = (spread - spread_top).astype(jnp.bfloat16)

    meta = jnp.stack([plane, place, planes - 1 - plane]).astype(jnp.int32)
    parts = flash(meta, slopes[0], lambdas[0], small_queries, large_queries, gathered)
    parts = parts.reshape(planes * core_count, row_count, -1)
    parts = lax.all_to_all(parts, OWNERS, split_axis=0, concat_axis=0, tiled=True)
    which = core.astype(jnp.int32).reshape(1)
    middle, keep, give = merge(
        which, parts, head_gain.reshape(1, -1), residual, out_weight, norm_gains[:1]
    )
    half = keep.shape[1]
    tokens = jnp.concatenate([keep, lax.ppermute(give, "tp", swap)], axis=0)
    outgoing = jnp.dot(selector, tokens, preferred_element_type=jnp.float32).astype(jnp.bfloat16)
    arrived = lax.all_to_all(
        outgoing.reshape(experts, block, half), SP, split_axis=0, concat_axis=0, tiled=True
    ).reshape(experts * block, half)
    sides = 2
    side_rows = experts * block // sides
    mine = [arrived[i * side_rows : (i + 1) * side_rows] for i in range(sides)]
    other = [lax.ppermute(rows, "tp", swap) for rows in mine]
    summed = []
    for i in range(sides):
        kept, given = expert(which, mine[i], other[i], gate_weight, up_weight, down_weight)
        got = lax.ppermute(given, "tp", swap)
        summed.append((kept.astype(jnp.float32) + got.astype(jnp.float32)).astype(jnp.bfloat16))
    returned = lax.all_to_all(
        jnp.concatenate(summed, axis=0).reshape(experts, block, half),
        SP,
        split_axis=0,
        concat_axis=0,
        tiled=True,
    ).reshape(experts * block, half)

    def weighed(first):
        cut = slice(first, first + row_count)
        return jnp.dot(spread_high[cut], returned, preferred_element_type=jnp.float32) + jnp.dot(
            spread_low[cut], returned, preferred_element_type=jnp.float32
        )

    received = lax.ppermute(weighed(row_count), "tp", swap)
    return final(which, weighed(0), received, middle, norm_gains[1:])


def solution(mesh):
    cube = Mesh(mesh.devices.reshape(4, 4, 4, 2), ("z", "y", "x", "tp"))
    both = SP + ("tp",)
    placed = (
        P(SP, "tp", None),
        P(SP, "tp", None),
        P(SP, "tp", None),
        P(SP, "tp", None),
        P(SP, "tp", None),
        P(SP, "tp", None),
        P("tp", None),
        P("tp", None),
        P(),
        P(both, None),
        P(),
        P(),
        P(both, None),
        P(both, None),
        P(SP, None, "tp"),
        P(SP, None, "tp"),
        P(SP, "tp", None),
    )
    return jax.shard_map(
        shards, mesh=cube, in_specs=placed, out_specs=P(both, None), check_vma=False
    )
```

```python
import jax
import jax.numpy as jnp
from jax import lax
from jax.experimental import pallas as pl
from jax.experimental.pallas import tpu as pltpu
from jax.sharding import Mesh, PartitionSpec as P

residual_gain = 8.0**0.25
epsilon = 1e-05
masked_score = -1e30
LOG2E = 1.4426950408889634
SP = ("z", "y", "x")
OWNERS = ("z", "tp")
SPAN = 2
LANES = 256
VMEM_LIMIT = 56 * 1024 * 1024


def three_parts(value):
    high = value.astype(jnp.bfloat16).astype(jnp.float32)
    rest = value - high
    middle = rest.astype(jnp.bfloat16).astype(jnp.float32)
    return high, middle, (rest - middle).astype(jnp.bfloat16).astype(jnp.float32)


def flash_body(meta, slope, lam, qt, *refs, first_axis, number):
    pieces, rest = refs[:5], refs[5:]
    prior = rest[0] if number else None
    out, keys, values, qs, bias, top, acc, sbuf, mbuf, tail = rest[number:]
    chunk, vsize = qt.shape[2], values.shape[1]
    width = qt.shape[1]
    half = width // 2
    place_count = keys.shape[0]
    side = 4
    plane, home_y, home_x = meta[0], meta[2], meta[3]
    place = home_y * side + home_x
    block = (meta[1] + pl.program_id(0)) % side
    scale = LOG2E * half ** (-0.5)
    slope_two = slope[0] * LOG2E
    rows = SPAN * chunk
    total = 2 * chunk

    @pl.when(pl.program_id(0) == 0)
    def _():
        slot = 0
        for piece in pieces:
            for i in range(piece.shape[0]):
                keys[slot] = piece[i, :, :width]
                values[slot] = piece[i, :, width:].T
                slot += 1

    qs[...] = jnp.zeros_like(qs)
    qs[:half, :chunk] = qt[0, :half, :]
    qs[half:, chunk:] = qt[0, half:, :]
    bias[...] = slope_two * lax.broadcasted_iota(jnp.int32, bias.shape, 0).astype(jnp.float32)
    top[...] = jnp.full_like(top, masked_score)
    acc[...] = jnp.zeros_like(acc)
    tail[...] = jnp.zeros_like(tail)
    last_query = (block - plane) * (place_count * chunk) + place * chunk + (chunk - 1)
    cuts = [slice(first, first + LANES) for first in range(0, total, LANES)]

    def slots_of(number):
        found = []
        for i in range(SPAN):
            spot = number * SPAN + i
            off_y = (spot // side - home_y + side) % side
            off_x = (spot % side - home_x + side) % side
            found.append(off_y * side + off_x if first_axis == "x" else off_x * side + off_y)
        return found

    def fill(number, slot):
        key_block = jnp.concatenate([keys[i] for i in slots_of(number)], axis=0)
        for cut in cuts:
            scores = jnp.dot(key_block, qs[:, cut], preferred_element_type=jnp.float32)
            scores = scores * scale + bias[...]
            sbuf[slot, :, cut] = scores
            mbuf[slot, :, cut] = jnp.max(scores, axis=0, keepdims=True)

    def use(number, slot):
        shift = slope_two * (number * rows - last_query).astype(jnp.float32)
        value_block = jnp.concatenate([values[i] for i in slots_of(number)], axis=1)
        value_block = jnp.concatenate([value_block, jnp.ones((16, rows), jnp.bfloat16)], axis=0)
        for cut in cuts:
            old = top[:, cut]
            new = jnp.maximum(old, mbuf[slot, :, cut] + shift)
            probs = jnp.exp2(sbuf[slot, :, cut] - (new - shift)).astype(jnp.bfloat16)
            top[:, cut] = new
            product = jnp.dot(value_block, probs, preferred_element_type=jnp.float32)
            acc[:, cut] = acc[:, cut] * jnp.exp2(old - new) + product

    def hide_later_keys(number, slot):
        for cut in cuts:
            lane = lax.broadcasted_iota(jnp.int32, (rows, LANES), 1) + cut.start
            lane = jnp.where(lane >= chunk, lane - chunk, lane)
            key_place = lax.broadcasted_iota(jnp.int32, (rows, LANES), 0) + number * rows
            scores = jnp.where(key_place <= lane + place * chunk, sbuf[slot, :, cut], masked_score)
            sbuf[slot, :, cut] = scores
            mbuf[slot, :, cut] = jnp.max(scores, axis=0, keepdims=True)

    most = place_count // SPAN
    count = jnp.where(block > plane, most, jnp.where(block == plane, place // SPAN + 1, 0))

    @pl.when(count > 0)
    def _():
        fill(0, 0)
        last = count - 1

        def pair_step(pair, carry):
            fill(2 * pair + 1, 1)
            use(2 * pair, 0)
            fill(jnp.minimum(2 * pair + 2, most - 1), 0)
            use(2 * pair + 1, 1)
            return carry

        lax.fori_loop(0, last // 2, pair_step, 0)

        @pl.when(last % 2 == 1)
        def _():
            fill(last, 1)
            use(last - 1, 0)

            @pl.when(block == plane)
            def _():
                hide_later_keys(last, 1)

            use(last, 1)

        @pl.when(last % 2 == 0)
        def _():
            @pl.when(block == plane)
            def _():
                hide_later_keys(last, 0)

            use(last, 0)

    sums = jnp.maximum(acc[vsize : vsize + 1, :], 1e-30)
    mixed = acc[:vsize, :] * (1.0 / sums)
    level = top[...] + jnp.log2(sums)
    lam_row = jnp.full((1, chunk), lam[0], jnp.float32)
    start = 2 * vsize * number
    for j in range(2):
        column = start + j * vsize
        out[0, :, column : column + vsize] = (
            mixed[:, j * chunk : (j + 1) * chunk].T.astype(jnp.bfloat16)
        )
        for k, part in enumerate(three_parts(level[:, j * chunk : (j + 1) * chunk])):
            row = 6 * k + 2 * number + j
            tail[row : row + 1, :] = part
    for k, part in enumerate(three_parts(lam_row)):
        row = 6 * k + 4 + number
        tail[row : row + 1, :] = part
    tails = tail[...].T
    if number:
        out[0, :, :start] = prior[0, :, :start]
        tails = tails + prior[0, :, start:].astype(jnp.float32)
    out[0, :, start + 2 * vsize :] = tails.astype(jnp.bfloat16)


def flash(number, meta, slope, lam, queries, pieces, prior, first_axis):
    blocks, _, chunk = queries.shape
    vsize = 128
    width = pieces[0].shape[2] - vsize
    place_count = sum(piece.shape[0] for piece in pieces)
    rows = SPAN * chunk
    q_row = 0 if number else 2
    lanes_out = 2 * vsize * (number + 1) + vsize
    scalar = pl.BlockSpec(memory_space=pltpu.SMEM)

    def own_block(b, meta):
        return ((meta[1] + b) % blocks, 0, 0)

    specs = [scalar, scalar, pl.BlockSpec((1, width, chunk), lambda b, meta: (b, q_row, 0))]
    specs += [pl.BlockSpec(piece.shape, lambda b, meta: (0, 0, 0)) for piece in pieces]
    operands = [slope, lam, queries, *pieces]
    if number:
        specs.append(pl.BlockSpec((1, chunk, prior.shape[2]), own_block))
        operands.append(prior)
    return pl.pallas_call(
        lambda *refs: flash_body(*refs, first_axis=first_axis, number=number),
        grid_spec=pltpu.PrefetchScalarGridSpec(
            num_scalar_prefetch=1,
            grid=(blocks,),
            in_specs=specs,
            out_specs=pl.BlockSpec((1, chunk, lanes_out), own_block),
            scratch_shapes=[
                pltpu.VMEM((place_count, chunk, width), jnp.bfloat16),
                pltpu.VMEM((place_count, vsize, chunk), jnp.bfloat16),
                pltpu.VMEM((width, 2 * chunk), jnp.bfloat16),
                pltpu.VMEM((rows, LANES), jnp.float32),
                pltpu.VMEM((1, 2 * chunk), jnp.float32),
                pltpu.VMEM((vsize + 16, 2 * chunk), jnp.float32),
                pltpu.VMEM((2, rows, 2 * chunk), jnp.float32),
                pltpu.VMEM((2, 1, 2 * chunk), jnp.float32),
                pltpu.VMEM((vsize, chunk), jnp.float32),
            ],
        ),
        out_shape=jax.ShapeDtypeStruct((blocks, chunk, lanes_out), jnp.bfloat16),
        compiler_params=pltpu.CompilerParams(
            dimension_semantics=("arbitrary",), vmem_limit_bytes=VMEM_LIMIT
        ),
    )(meta, *operands)


def around(value, axis):
    size = lax.axis_size(axis)
    cut = value.shape[0] // 2
    ahead = [((i + 1) % size, i) for i in range(size)]
    behind = [((i - 1) % size, i) for i in range(size)]
    one = lax.ppermute(value, axis, ahead)
    three = lax.ppermute(value, axis, behind)
    two_first = lax.ppermute(one[:cut], axis, ahead)
    two_last = lax.ppermute(three[cut:], axis, behind)
    return [value, one, two_first, two_last, three]


def normed(values, gain_row):
    average = jnp.mean(values, axis=-1, keepdims=True)
    centred = values - average
    variance = jnp.mean(centred * centred, axis=-1, keepdims=True)
    return centred * lax.rsqrt(variance + epsilon) * gain_row


def merge_body(core, arrived, head_gain, residual, weight, norm_gain, middle, keep, give):
    planes = arrived.shape[0] // 2
    vsize = head_gain.shape[1]
    gain = head_gain[...].astype(jnp.float32)
    pieces = []
    for head in range(2):
        tails = []
        for z in range(planes):
            lanes = arrived[2 * z + head, :, 4 * vsize :].astype(jnp.float32)
            tails.append([lanes[:, i : i + 1] + lanes[:, i + 6 : i + 7] + lanes[:, i + 12 : i + 13] for i in range(6)])
        for group in range(2):
            mixtures = []
            for j in range(2):
                index = 2 * group + j
                highest = tails[0][index]
                for z in range(1, planes):
                    highest = jnp.maximum(highest, tails[z][index])
                weights = [jnp.exp2(tails[z][index] - highest) for z in range(planes)]
                scaled = 1.0 / sum(weights)
                column = index * vsize
                mixtures.append(
                    sum(
                        (weights[z] * scaled)
                        * arrived[2 * z + head, :, column : column + vsize].astype(jnp.float32)
                        for z in range(planes)
                    )
                )
            head_out = mixtures[0] - tails[0][4 + group] * mixtures[1]
            power = jnp.mean(head_out * head_out, axis=-1, keepdims=True)
            pieces.append((head_out * lax.rsqrt(power + epsilon) * gain).astype(jnp.bfloat16))
    attended = jnp.concatenate(pieces, axis=1)
    projected = jnp.dot(attended, weight[...], preferred_element_type=jnp.float32)
    values = residual_gain * residual[...].astype(jnp.float32) + projected
    result = normed(values, norm_gain[...].astype(jnp.float32)).astype(jnp.bfloat16)
    middle[...] = result
    half = result.shape[1] // 2

    @pl.when(core[0] == 0)
    def _():
        keep[...] = result[:, :half]
        give[...] = result[:, half:]

    @pl.when(core[0] == 1)
    def _():
        keep[...] = result[:, half:]
        give[...] = result[:, :half]


def merge(core, arrived, head_gain, residual, weight, norm_gain):
    count, features = residual.shape
    return pl.pallas_call(
        merge_body,
        in_specs=[pl.BlockSpec(memory_space=pltpu.SMEM)] + [pl.BlockSpec(memory_space=pltpu.VMEM)] * 5,
        out_shape=[
            jax.ShapeDtypeStruct((count, features), jnp.bfloat16),
            jax.ShapeDtypeStruct((count, features // 2), jnp.bfloat16),
            jax.ShapeDtypeStruct((count, features // 2), jnp.bfloat16),
        ],
        compiler_params=pltpu.CompilerParams(vmem_limit_bytes=VMEM_LIMIT),
    )(core, arrived, head_gain, residual, weight, norm_gain)


def expert_body(core, mine, other, gate, up, down, keep, give):
    half = mine.shape[1]
    first = pl.multiple_of(core[0] * half, half)
    second = pl.multiple_of((1 - core[0]) * half, half)
    own_rows = mine[...]
    other_rows = other[...]

    def through(weight):
        return jnp.dot(
            own_rows, weight[0, pl.ds(first, half), :], preferred_element_type=jnp.float32
        ) + jnp.dot(
            other_rows, weight[0, pl.ds(second, half), :], preferred_element_type=jnp.float32
        )

    gate_in = through(gate)
    upward = through(up)
    hidden = (gate_in * (1.0 / (1.0 + jnp.exp(-gate_in))) * upward).astype(jnp.bfloat16)
    keep[...] = jnp.dot(
        hidden, down[0, :, pl.ds(first, half)], preferred_element_type=jnp.float32
    ).astype(jnp.bfloat16)
    give[...] = jnp.dot(
        hidden, down[0, :, pl.ds(second, half)], preferred_element_type=jnp.float32
    ).astype(jnp.bfloat16)


def expert(core, mine, other, gate, up, down):
    count, half = mine.shape
    block_rows = 256
    rows = pl.BlockSpec((block_rows, half), lambda i: (i, 0))
    shape = jax.ShapeDtypeStruct((count, half), jnp.bfloat16)
    return pl.pallas_call(
        expert_body,
        grid=(count // block_rows,),
        in_specs=[
            pl.BlockSpec(memory_space=pltpu.SMEM),
            rows,
            rows,
            pl.BlockSpec(gate.shape, lambda i: (0, 0, 0)),
            pl.BlockSpec(up.shape, lambda i: (0, 0, 0)),
            pl.BlockSpec(down.shape, lambda i: (0, 0, 0)),
        ],
        out_specs=[rows, rows],
        out_shape=[shape, shape],
        compiler_params=pltpu.CompilerParams(
            dimension_semantics=("arbitrary",), vmem_limit_bytes=VMEM_LIMIT
        ),
    )(core, mine, other, gate, up, down)


def final_body(core, own, received, middle, norm_gain, out, total):
    half = own.shape[1]

    @pl.when(core[0] == 0)
    def _():
        total[:, :half] = own[...]
        total[:, half:] = received[...]

    @pl.when(core[0] == 1)
    def _():
        total[:, :half] = received[...]
        total[:, half:] = own[...]

    values = residual_gain * middle[...].astype(jnp.float32) + total[...]
    out[...] = normed(values, norm_gain[...].astype(jnp.float32)).astype(jnp.bfloat16)


def final(core, own, received, middle, norm_gain):
    return pl.pallas_call(
        final_body,
        in_specs=[pl.BlockSpec(memory_space=pltpu.SMEM)] + [pl.BlockSpec(memory_space=pltpu.VMEM)] * 4,
        out_shape=jax.ShapeDtypeStruct(middle.shape, jnp.bfloat16),
        scratch_shapes=[pltpu.VMEM(middle.shape, jnp.float32)],
        compiler_params=pltpu.CompilerParams(vmem_limit_bytes=VMEM_LIMIT),
    )(core, own, received, middle, norm_gain)


def slots(routes, experts, block, offset):
    chosen = routes.reshape(-1)
    matches = (chosen[:, None] == jnp.arange(experts)[None, :]).astype(jnp.int32)
    earlier = jnp.cumsum(matches, axis=0) - matches
    rank = jnp.sum(earlier * matches, axis=1)
    return (chosen * block + offset + rank).reshape(routes.shape)


def shards(
    query_small,
    key_small,
    value_small,
    query_large,
    key_large,
    value_large,
    lambdas,
    slopes,
    head_gain,
    residual,
    out_weight,
    norm_gains,
    routes,
    route_weights,
    gate_weight,
    up_weight,
    down_weight,
):
    length = query_small.shape[0]
    planes = lax.axis_size("z")
    plane = lax.axis_index("z")
    core = lax.axis_index("tp")
    mirror = [(i, planes - 1 - i) for i in range(planes)]
    swap = [(0, 1), (1, 0)]
    small_pack = jnp.concatenate(
        [key_small.reshape(length, -1), value_small.reshape(length, -1)], axis=1
    )
    large_pack = jnp.concatenate(
        [key_large.reshape(length, -1), value_large.reshape(length, -1)], axis=1
    )
    query_pack = jnp.concatenate(
        [query_large.reshape(length, -1).T, query_small.reshape(length, -1).T], axis=0
    )
    small_pack = lax.ppermute(small_pack, "z", mirror)
    queries = jnp.concatenate(around(query_pack, "z"), axis=0).reshape(planes, *query_pack.shape)
    large_row = jnp.concatenate(around(large_pack, "x"), axis=0).reshape(4, *large_pack.shape)
    small_row = jnp.concatenate(around(small_pack, "y"), axis=0).reshape(4, *small_pack.shape)
    small_pieces = around(small_row, "x")
    large_pieces = around(large_row, "y")

    core_count = lax.axis_size("tp")
    row_count = length // core_count
    experts = lax.axis_size(SP)
    block = core_count * (4 * row_count // experts)
    their_routes = lax.ppermute(routes, "tp", swap)
    their_weights = lax.ppermute(route_weights, "tp", swap)
    capacity = block // core_count
    target = jnp.concatenate(
        [
            slots(routes, experts, block, core * capacity),
            slots(their_routes, experts, block, (1 - core) * capacity),
        ],
        axis=0,
    )
    shares = jnp.concatenate([route_weights, their_weights], axis=0)
    places = jnp.arange(experts * block)
    hits = [target[:, k] for k in range(2)]
    selector = (
        (hits[0][None, :] == places[:, None]) | (hits[1][None, :] == places[:, None])
    ).astype(jnp.bfloat16)
    spread = jnp.where(hits[0][:, None] == places[None, :], shares[:, :1], 0.0) + jnp.where(
        hits[1][:, None] == places[None, :], shares[:, 1:], 0.0
    )
    spread_top = lax.reduce_precision(spread, exponent_bits=8, mantissa_bits=7)
    spread_high = spread_top.astype(jnp.bfloat16)
    spread_low = (spread - spread_top).astype(jnp.bfloat16)

    home = [plane, lax.axis_index("y"), lax.axis_index("x")]
    small_meta = jnp.stack([planes - 1 - plane, *home]).astype(jnp.int32)
    large_meta = jnp.stack([plane, *home]).astype(jnp.int32)
    parts = flash(
        0, small_meta, slopes[0, :1], lambdas[0, :1], queries, small_pieces, None, "y"
    )
    parts = flash(
        1, large_meta, slopes[0, 1:], lambdas[0, 1:], queries, large_pieces, parts, "x"
    )
    parts = parts.reshape(planes * core_count, row_count, -1)
    parts = lax.all_to_all(parts, OWNERS, split_axis=0, concat_axis=0, tiled=True)
    which = core.astype(jnp.int32).reshape(1)
    middle, keep, give = merge(
        which, parts, head_gain.reshape(1, -1), residual, out_weight, norm_gains[:1]
    )
    half = keep.shape[1]
    tokens = jnp.concatenate([keep, lax.ppermute(give, "tp", swap)], axis=0)
    outgoing = jnp.dot(selector, tokens, preferred_element_type=jnp.float32).astype(jnp.bfloat16)
    arrived = lax.all_to_all(
        outgoing.reshape(experts, block, half), SP, split_axis=0, concat_axis=0, tiled=True
    ).reshape(experts * block, half)
    sides = 2
    side_rows = experts * block // sides
    mine = [arrived[i * side_rows : (i + 1) * side_rows] for i in range(sides)]
    other = [lax.ppermute(rows, "tp", swap) for rows in mine]
    summed = []
    for i in range(sides):
        kept, given = expert(which, mine[i], other[i], gate_weight, up_weight, down_weight)
        got = lax.ppermute(given, "tp", swap)
        summed.append((kept.astype(jnp.float32) + got.astype(jnp.float32)).astype(jnp.bfloat16))
    returned = lax.all_to_all(
        jnp.concatenate(summed, axis=0).reshape(experts, block, half),
        SP,
        split_axis=0,
        concat_axis=0,
        tiled=True,
    ).reshape(experts * block, half)

    def weighed(first):
        cut = slice(first, first + row_count)
        return jnp.dot(spread_high[cut], returned, preferred_element_type=jnp.float32) + jnp.dot(
            spread_low[cut], returned, preferred_element_type=jnp.float32
        )

    received = lax.ppermute(weighed(row_count), "tp", swap)
    return final(which, weighed(0), received, middle, norm_gains[1:])


def solution(mesh):
    cube = Mesh(mesh.devices.reshape(4, 4, 4, 2), ("z", "y", "x", "tp"))
    both = SP + ("tp",)
    placed = (
        P(SP, "tp", None),
        P(SP, "tp", None),
        P(SP, "tp", None),
        P(SP, "tp", None),
        P(SP, "tp", None),
        P(SP, "tp", None),
        P("tp", None),
        P("tp", None),
        P(),
        P(both, None),
        P(),
        P(),
        P(both, None),
        P(both, None),
        P(SP, None, "tp"),
        P(SP, None, "tp"),
        P(SP, "tp", None),
    )
    return jax.shard_map(
        shards, mesh=cube, in_specs=placed, out_specs=P(both, None), check_vma=False
    )
```

```python
import jax
import jax.numpy as jnp
from jax import lax
from jax.experimental import pallas as pl
from jax.experimental.pallas import tpu as pltpu
from jax.sharding import Mesh, PartitionSpec as P

residual_gain = 8.0**0.25
epsilon = 1e-05
masked_score = -1e30
LOG2E = 1.4426950408889634
SP = ("z", "y", "x")
OWNERS = ("z", "tp")
SPAN = 2
LANES = 256
VMEM_LIMIT = 56 * 1024 * 1024


def three_parts(value):
    high = value.astype(jnp.bfloat16).astype(jnp.float32)
    rest = value - high
    middle = rest.astype(jnp.bfloat16).astype(jnp.float32)
    return high, middle, (rest - middle).astype(jnp.bfloat16).astype(jnp.float32)


def flash_body(meta, slope, lam, qt, *refs, first_axis, number):
    pieces, rest = refs[:5], refs[5:]
    prior = rest[0] if number else None
    out, keys, values, qs, bias, top, acc, sbuf, mbuf, tail = rest[number:]
    chunk, vsize = qt.shape[2], values.shape[1]
    width = qt.shape[1]
    half = width // 2
    place_count = keys.shape[0]
    side = 4
    plane, home_y, home_x = meta[0], meta[2], meta[3]
    place = home_y * side + home_x
    block = (meta[1] + pl.program_id(0)) % side
    scale = LOG2E * half ** (-0.5)
    slope_two = slope[0] * LOG2E
    rows = SPAN * chunk
    total = 2 * chunk

    @pl.when(pl.program_id(0) == 0)
    def _():
        slot = 0
        for piece in pieces:
            for i in range(piece.shape[0]):
                keys[slot] = piece[i, :, :width]
                values[slot] = piece[i, :, width:].T
                slot += 1

    qs[...] = jnp.zeros_like(qs)
    qs[:half, :chunk] = qt[0, :half, :]
    qs[half:, chunk:] = qt[0, half:, :]
    bias[...] = slope_two * lax.broadcasted_iota(jnp.int32, bias.shape, 0).astype(jnp.float32)
    top[...] = jnp.full_like(top, masked_score)
    acc[...] = jnp.zeros_like(acc)
    tail[...] = jnp.zeros_like(tail)
    last_query = (block - plane) * (place_count * chunk) + place * chunk + (chunk - 1)
    cuts = [slice(first, first + LANES) for first in range(0, total, LANES)]

    def slots_of(number):
        found = []
        for i in range(SPAN):
            spot = number * SPAN + i
            off_y = (spot // side - home_y + side) % side
            off_x = (spot % side - home_x + side) % side
            found.append(off_y * side + off_x if first_axis == "x" else off_x * side + off_y)
        return found

    def fill(number, slot):
        key_block = jnp.concatenate([keys[i] for i in slots_of(number)], axis=0)
        for cut in cuts:
            scores = jnp.dot(key_block, qs[:, cut], preferred_element_type=jnp.float32)
            scores = scores * scale + bias[...]
            sbuf[slot, :, cut] = scores
            mbuf[slot, :, cut] = jnp.max(scores, axis=0, keepdims=True)

    def use(number, slot):
        shift = slope_two * (number * rows - last_query).astype(jnp.float32)
        value_block = jnp.concatenate([values[i] for i in slots_of(number)], axis=1)
        value_block = jnp.concatenate([value_block, jnp.ones((16, rows), jnp.bfloat16)], axis=0)
        for cut in cuts:
            old = top[:, cut]
            new = jnp.maximum(old, mbuf[slot, :, cut] + shift)
            probs = jnp.exp2(sbuf[slot, :, cut] - (new - shift)).astype(jnp.bfloat16)
            top[:, cut] = new
            product = jnp.dot(value_block, probs, preferred_element_type=jnp.float32)
            acc[:, cut] = acc[:, cut] * jnp.exp2(old - new) + product

    def hide_later_keys(number, slot):
        for cut in cuts:
            lane = lax.broadcasted_iota(jnp.int32, (rows, LANES), 1) + cut.start
            lane = jnp.where(lane >= chunk, lane - chunk, lane)
            key_place = lax.broadcasted_iota(jnp.int32, (rows, LANES), 0) + number * rows
            scores = jnp.where(key_place <= lane + place * chunk, sbuf[slot, :, cut], masked_score)
            sbuf[slot, :, cut] = scores
            mbuf[slot, :, cut] = jnp.max(scores, axis=0, keepdims=True)

    most = place_count // SPAN
    count = jnp.where(block > plane, most, jnp.where(block == plane, place // SPAN + 1, 0))

    @pl.when(count > 0)
    def _():
        fill(0, 0)
        last = count - 1

        def pair_step(pair, carry):
            fill(2 * pair + 1, 1)
            use(2 * pair, 0)
            fill(jnp.minimum(2 * pair + 2, most - 1), 0)
            use(2 * pair + 1, 1)
            return carry

        lax.fori_loop(0, last // 2, pair_step, 0)

        @pl.when(last % 2 == 1)
        def _():
            fill(last, 1)
            use(last - 1, 0)

            @pl.when(block == plane)
            def _():
                hide_later_keys(last, 1)

            use(last, 1)

        @pl.when(last % 2 == 0)
        def _():
            @pl.when(block == plane)
            def _():
                hide_later_keys(last, 0)

            use(last, 0)

    sums = jnp.maximum(acc[vsize : vsize + 1, :], 1e-30)
    mixed = acc[:vsize, :] * (1.0 / sums)
    level = top[...] + jnp.log2(sums)
    lam_row = jnp.full((1, chunk), lam[0], jnp.float32)
    start = 2 * vsize * number
    for j in range(2):
        column = start + j * vsize
        out[0, :, column : column + vsize] = (
            mixed[:, j * chunk : (j + 1) * chunk].T.astype(jnp.bfloat16)
        )
        for k, part in enumerate(three_parts(level[:, j * chunk : (j + 1) * chunk])):
            row = 6 * k + 2 * number + j
            tail[row : row + 1, :] = part
    for k, part in enumerate(three_parts(lam_row)):
        row = 6 * k + 4 + number
        tail[row : row + 1, :] = part
    tails = tail[...].T
    if number:
        out[0, :, :start] = prior[0, :, :start]
        tails = tails + prior[0, :, start:].astype(jnp.float32)
    out[0, :, start + 2 * vsize :] = tails.astype(jnp.bfloat16)


def flash(number, meta, slope, lam, queries, pieces, prior, first_axis):
    blocks, _, chunk = queries.shape
    vsize = 128
    width = pieces[0].shape[2] - vsize
    place_count = sum(piece.shape[0] for piece in pieces)
    rows = SPAN * chunk
    q_row = 0 if number else 2
    lanes_out = 2 * vsize * (number + 1) + vsize
    scalar = pl.BlockSpec(memory_space=pltpu.SMEM)

    def own_block(b, meta):
        return ((meta[1] + b) % blocks, 0, 0)

    specs = [scalar, scalar, pl.BlockSpec((1, width, chunk), lambda b, meta: (b, q_row, 0))]
    specs += [pl.BlockSpec(piece.shape, lambda b, meta: (0, 0, 0)) for piece in pieces]
    operands = [slope, lam, queries, *pieces]
    if number:
        specs.append(pl.BlockSpec((1, chunk, prior.shape[2]), own_block))
        operands.append(prior)
    return pl.pallas_call(
        lambda *refs: flash_body(*refs, first_axis=first_axis, number=number),
        grid_spec=pltpu.PrefetchScalarGridSpec(
            num_scalar_prefetch=1,
            grid=(blocks,),
            in_specs=specs,
            out_specs=pl.BlockSpec((1, chunk, lanes_out), own_block),
            scratch_shapes=[
                pltpu.VMEM((place_count, chunk, width), jnp.bfloat16),
                pltpu.VMEM((place_count, vsize, chunk), jnp.bfloat16),
                pltpu.VMEM((width, 2 * chunk), jnp.bfloat16),
                pltpu.VMEM((rows, LANES), jnp.float32),
                pltpu.VMEM((1, 2 * chunk), jnp.float32),
                pltpu.VMEM((vsize + 16, 2 * chunk), jnp.float32),
                pltpu.VMEM((2, rows, 2 * chunk), jnp.float32),
                pltpu.VMEM((2, 1, 2 * chunk), jnp.float32),
                pltpu.VMEM((vsize, chunk), jnp.float32),
            ],
        ),
        out_shape=jax.ShapeDtypeStruct((blocks, chunk, lanes_out), jnp.bfloat16),
        cost_estimate=pl.CostEstimate(flops=20_000_000_000, transcendentals=0, bytes_accessed=0),
        compiler_params=pltpu.CompilerParams(
            dimension_semantics=("arbitrary",), vmem_limit_bytes=VMEM_LIMIT
        ),
    )(meta, *operands)


def around(value, axis):
    size = lax.axis_size(axis)
    cut = value.shape[0] // 2
    ahead = [((i + 1) % size, i) for i in range(size)]
    behind = [((i - 1) % size, i) for i in range(size)]
    one = lax.ppermute(value, axis, ahead)
    three = lax.ppermute(value, axis, behind)
    two_first = lax.ppermute(one[:cut], axis, ahead)
    two_last = lax.ppermute(three[cut:], axis, behind)
    return [value, one, two_first, two_last, three]


def normed(values, gain_row):
    average = jnp.mean(values, axis=-1, keepdims=True)
    centred = values - average
    variance = jnp.mean(centred * centred, axis=-1, keepdims=True)
    return centred * lax.rsqrt(variance + epsilon) * gain_row


def merge_body(core, arrived, head_gain, residual, weight, norm_gain, middle, keep, give):
    planes = arrived.shape[0] // 2
    vsize = head_gain.shape[1]
    gain = head_gain[...].astype(jnp.float32)
    pieces = []
    for head in range(2):
        tails = []
        for z in range(planes):
            lanes = arrived[2 * z + head, :, 4 * vsize :].astype(jnp.float32)
            tails.append([lanes[:, i : i + 1] + lanes[:, i + 6 : i + 7] + lanes[:, i + 12 : i + 13] for i in range(6)])
        for group in range(2):
            mixtures = []
            for j in range(2):
                index = 2 * group + j
                highest = tails[0][index]
                for z in range(1, planes):
                    highest = jnp.maximum(highest, tails[z][index])
                weights = [jnp.exp2(tails[z][index] - highest) for z in range(planes)]
                scaled = 1.0 / sum(weights)
                column = index * vsize
                mixtures.append(
                    sum(
                        (weights[z] * scaled)
                        * arrived[2 * z + head, :, column : column + vsize].astype(jnp.float32)
                        for z in range(planes)
                    )
                )
            head_out = mixtures[0] - tails[0][4 + group] * mixtures[1]
            power = jnp.mean(head_out * head_out, axis=-1, keepdims=True)
            pieces.append((head_out * lax.rsqrt(power + epsilon) * gain).astype(jnp.bfloat16))
    attended = jnp.concatenate(pieces, axis=1)
    projected = jnp.dot(attended, weight[...], preferred_element_type=jnp.float32)
    values = residual_gain * residual[...].astype(jnp.float32) + projected
    result = normed(values, norm_gain[...].astype(jnp.float32)).astype(jnp.bfloat16)
    middle[...] = result
    half = result.shape[1] // 2

    @pl.when(core[0] == 0)
    def _():
        keep[...] = result[:, :half]
        give[...] = result[:, half:]

    @pl.when(core[0] == 1)
    def _():
        keep[...] = result[:, half:]
        give[...] = result[:, :half]


def merge(core, arrived, head_gain, residual, weight, norm_gain):
    count, features = residual.shape
    return pl.pallas_call(
        merge_body,
        in_specs=[pl.BlockSpec(memory_space=pltpu.SMEM)] + [pl.BlockSpec(memory_space=pltpu.VMEM)] * 5,
        out_shape=[
            jax.ShapeDtypeStruct((count, features), jnp.bfloat16),
            jax.ShapeDtypeStruct((count, features // 2), jnp.bfloat16),
            jax.ShapeDtypeStruct((count, features // 2), jnp.bfloat16),
        ],
        cost_estimate=pl.CostEstimate(flops=5_000_000_000, transcendentals=0, bytes_accessed=0),
        compiler_params=pltpu.CompilerParams(vmem_limit_bytes=VMEM_LIMIT),
    )(core, arrived, head_gain, residual, weight, norm_gain)


def expert_body(core, mine, other, gate, up, down, keep, give):
    half = mine.shape[1]
    first = pl.multiple_of(core[0] * half, half)
    second = pl.multiple_of((1 - core[0]) * half, half)
    own_rows = mine[...]
    other_rows = other[...]

    def through(weight):
        return jnp.dot(
            own_rows, weight[0, pl.ds(first, half), :], preferred_element_type=jnp.float32
        ) + jnp.dot(
            other_rows, weight[0, pl.ds(second, half), :], preferred_element_type=jnp.float32
        )

    gate_in = through(gate)
    upward = through(up)
    hidden = (gate_in * (1.0 / (1.0 + jnp.exp(-gate_in))) * upward).astype(jnp.bfloat16)
    keep[...] = jnp.dot(
        hidden, down[0, :, pl.ds(first, half)], preferred_element_type=jnp.float32
    ).astype(jnp.bfloat16)
    give[...] = jnp.dot(
        hidden, down[0, :, pl.ds(second, half)], preferred_element_type=jnp.float32
    ).astype(jnp.bfloat16)


def expert(core, mine, other, gate, up, down):
    count, half = mine.shape
    block_rows = 256
    rows = pl.BlockSpec((block_rows, half), lambda i: (i, 0))
    shape = jax.ShapeDtypeStruct((count, half), jnp.bfloat16)
    return pl.pallas_call(
        expert_body,
        grid=(count // block_rows,),
        in_specs=[
            pl.BlockSpec(memory_space=pltpu.SMEM),
            rows,
            rows,
            pl.BlockSpec(gate.shape, lambda i: (0, 0, 0)),
            pl.BlockSpec(up.shape, lambda i: (0, 0, 0)),
            pl.BlockSpec(down.shape, lambda i: (0, 0, 0)),
        ],
        out_specs=[rows, rows],
        out_shape=[shape, shape],
        cost_estimate=pl.CostEstimate(flops=count * 12_000_000, transcendentals=0, bytes_accessed=0),
        compiler_params=pltpu.CompilerParams(
            dimension_semantics=("arbitrary",), vmem_limit_bytes=VMEM_LIMIT
        ),
    )(core, mine, other, gate, up, down)


def final_body(core, own, received, middle, norm_gain, out, total):
    half = own.shape[1]

    @pl.when(core[0] == 0)
    def _():
        total[:, :half] = own[...]
        total[:, half:] = received[...]

    @pl.when(core[0] == 1)
    def _():
        total[:, :half] = received[...]
        total[:, half:] = own[...]

    values = residual_gain * middle[...].astype(jnp.float32) + total[...]
    out[...] = normed(values, norm_gain[...].astype(jnp.float32)).astype(jnp.bfloat16)


def final(core, own, received, middle, norm_gain):
    return pl.pallas_call(
        final_body,
        in_specs=[pl.BlockSpec(memory_space=pltpu.SMEM)] + [pl.BlockSpec(memory_space=pltpu.VMEM)] * 4,
        out_shape=jax.ShapeDtypeStruct(middle.shape, jnp.bfloat16),
        scratch_shapes=[pltpu.VMEM(middle.shape, jnp.float32)],
        cost_estimate=pl.CostEstimate(flops=2_000_000_000, transcendentals=0, bytes_accessed=0),
        compiler_params=pltpu.CompilerParams(vmem_limit_bytes=VMEM_LIMIT),
    )(core, own, received, middle, norm_gain)


def slots(routes, experts, block, offset):
    chosen = routes.reshape(-1)
    matches = (chosen[:, None] == jnp.arange(experts)[None, :]).astype(jnp.int32)
    earlier = jnp.cumsum(matches, axis=0) - matches
    rank = jnp.sum(earlier * matches, axis=1)
    return (chosen * block + offset + rank).reshape(routes.shape)


def shards(
    query_small,
    key_small,
    value_small,
    query_large,
    key_large,
    value_large,
    lambdas,
    slopes,
    head_gain,
    residual,
    out_weight,
    norm_gains,
    routes,
    route_weights,
    gate_weight,
    up_weight,
    down_weight,
):
    length = query_small.shape[0]
    planes = lax.axis_size("z")
    plane = lax.axis_index("z")
    core = lax.axis_index("tp")
    mirror = [(i, planes - 1 - i) for i in range(planes)]
    swap = [(0, 1), (1, 0)]
    small_pack = jnp.concatenate(
        [key_small.reshape(length, -1), value_small.reshape(length, -1)], axis=1
    )
    large_pack = jnp.concatenate(
        [key_large.reshape(length, -1), value_large.reshape(length, -1)], axis=1
    )
    query_pack = jnp.concatenate(
        [query_large.reshape(length, -1).T, query_small.reshape(length, -1).T], axis=0
    )
    small_pack = lax.ppermute(small_pack, "z", mirror)
    queries = jnp.concatenate(around(query_pack, "z"), axis=0).reshape(planes, *query_pack.shape)
    large_row = jnp.concatenate(around(large_pack, "x"), axis=0).reshape(4, *large_pack.shape)
    small_row = jnp.concatenate(around(small_pack, "y"), axis=0).reshape(4, *small_pack.shape)
    large_row, small_row, queries = lax.optimization_barrier((large_row, small_row, queries))
    small_pieces = around(small_row, "x")
    large_pieces = around(large_row, "y")

    core_count = lax.axis_size("tp")
    row_count = length // core_count
    experts = lax.axis_size(SP)
    block = core_count * (4 * row_count // experts)
    their_routes = lax.ppermute(routes, "tp", swap)
    their_weights = lax.ppermute(route_weights, "tp", swap)
    capacity = block // core_count
    target = jnp.concatenate(
        [
            slots(routes, experts, block, core * capacity),
            slots(their_routes, experts, block, (1 - core) * capacity),
        ],
        axis=0,
    )
    shares = jnp.concatenate([route_weights, their_weights], axis=0)
    places = jnp.arange(experts * block)
    hits = [target[:, k] for k in range(2)]
    selector = (
        (hits[0][None, :] == places[:, None]) | (hits[1][None, :] == places[:, None])
    ).astype(jnp.bfloat16)
    spread = jnp.where(hits[0][:, None] == places[None, :], shares[:, :1], 0.0) + jnp.where(
        hits[1][:, None] == places[None, :], shares[:, 1:], 0.0
    )
    spread_top = lax.reduce_precision(spread, exponent_bits=8, mantissa_bits=7)
    spread_high = spread_top.astype(jnp.bfloat16)
    spread_low = (spread - spread_top).astype(jnp.bfloat16)

    home = [plane, lax.axis_index("y"), lax.axis_index("x")]
    small_meta = jnp.stack([planes - 1 - plane, *home]).astype(jnp.int32)
    large_meta = jnp.stack([plane, *home]).astype(jnp.int32)
    parts = flash(
        0, small_meta, slopes[0, :1], lambdas[0, :1], queries, small_pieces, None, "y"
    )
    parts = flash(
        1, large_meta, slopes[0, 1:], lambdas[0, 1:], queries, large_pieces, parts, "x"
    )
    parts = parts.reshape(planes * core_count, row_count, -1)
    parts = lax.all_to_all(parts, OWNERS, split_axis=0, concat_axis=0, tiled=True)
    which = core.astype(jnp.int32).reshape(1)
    middle, keep, give = merge(
        which, parts, head_gain.reshape(1, -1), residual, out_weight, norm_gains[:1]
    )
    half = keep.shape[1]
    tokens = jnp.concatenate([keep, lax.ppermute(give, "tp", swap)], axis=0)
    outgoing = jnp.dot(selector, tokens, preferred_element_type=jnp.float32).astype(jnp.bfloat16)
    arrived = lax.all_to_all(
        outgoing.reshape(experts, block, half), SP, split_axis=0, concat_axis=0, tiled=True
    ).reshape(experts * block, half)
    sides = 2
    side_rows = experts * block // sides
    mine = [arrived[i * side_rows : (i + 1) * side_rows] for i in range(sides)]
    other = [lax.ppermute(rows, "tp", swap) for rows in mine]
    summed = []
    for i in range(sides):
        kept, given = expert(which, mine[i], other[i], gate_weight, up_weight, down_weight)
        got = lax.ppermute(given, "tp", swap)
        summed.append((kept.astype(jnp.float32) + got.astype(jnp.float32)).astype(jnp.bfloat16))
    returned = lax.all_to_all(
        jnp.concatenate(summed, axis=0).reshape(experts, block, half),
        SP,
        split_axis=0,
        concat_axis=0,
        tiled=True,
    ).reshape(experts * block, half)

    def weighed(first):
        cut = slice(first, first + row_count)
        return jnp.dot(spread_high[cut], returned, preferred_element_type=jnp.float32) + jnp.dot(
            spread_low[cut], returned, preferred_element_type=jnp.float32
        )

    received = lax.ppermute(weighed(row_count), "tp", swap)
    return final(which, weighed(0), received, middle, norm_gains[1:])


def solution(mesh):
    cube = Mesh(mesh.devices.reshape(4, 4, 4, 2), ("z", "y", "x", "tp"))
    both = SP + ("tp",)
    placed = (
        P(SP, "tp", None),
        P(SP, "tp", None),
        P(SP, "tp", None),
        P(SP, "tp", None),
        P(SP, "tp", None),
        P(SP, "tp", None),
        P("tp", None),
        P("tp", None),
        P(),
        P(both, None),
        P(),
        P(),
        P(both, None),
        P(both, None),
        P(SP, None, "tp"),
        P(SP, None, "tp"),
        P(SP, "tp", None),
    )
    return jax.shard_map(
        shards, mesh=cube, in_specs=placed, out_specs=P(both, None), check_vma=False
    )
```

```python
import jax
import jax.numpy as jnp
from jax import lax
from jax.experimental import pallas as pl
from jax.experimental.pallas import tpu as pltpu
from jax.sharding import Mesh, PartitionSpec as P

residual_gain = 8.0**0.25
epsilon = 1e-05
masked_score = -1e30
LOG2E = 1.4426950408889634
SP = ("z", "y", "x")
OWNERS = ("z", "tp")
SPAN = 2
LANES = 256
VMEM_LIMIT = 56 * 1024 * 1024


def three_parts(value):
    high = value.astype(jnp.bfloat16).astype(jnp.float32)
    rest = value - high
    middle = rest.astype(jnp.bfloat16).astype(jnp.float32)
    return high, middle, (rest - middle).astype(jnp.bfloat16).astype(jnp.float32)


def flash_body(meta, slope, lam, qt, *refs, first_axis, number):
    pieces, rest = refs[:5], refs[5:]
    prior = rest[0] if number else None
    out, keys, values, qs, bias, top, acc, sbuf, mbuf, tail = rest[number:]
    chunk, vsize = qt.shape[2], values.shape[1]
    width = qt.shape[1]
    half = width // 2
    place_count = keys.shape[0]
    side = 4
    plane, home_y, home_x = meta[0], meta[2], meta[3]
    place = home_y * side + home_x
    block = (meta[1] + pl.program_id(0)) % side
    scale = LOG2E * half ** (-0.5)
    slope_two = slope[0] * LOG2E
    rows = SPAN * chunk
    total = 2 * chunk

    @pl.when(pl.program_id(0) == 0)
    def _():
        slot = 0
        for piece in pieces:
            for i in range(piece.shape[0]):
                keys[slot] = piece[i, :, :width]
                values[slot] = piece[i, :, width:].T
                slot += 1

    qs[...] = jnp.zeros_like(qs)
    qs[:half, :chunk] = qt[0, :half, :]
    qs[half:, chunk:] = qt[0, half:, :]
    bias[...] = slope_two * lax.broadcasted_iota(jnp.int32, bias.shape, 0).astype(jnp.float32)
    top[...] = jnp.full_like(top, masked_score)
    acc[...] = jnp.zeros_like(acc)
    tail[...] = jnp.zeros_like(tail)
    last_query = (block - plane) * (place_count * chunk) + place * chunk + (chunk - 1)
    cuts = [slice(first, first + LANES) for first in range(0, total, LANES)]

    def slots_of(number):
        found = []
        for i in range(SPAN):
            spot = number * SPAN + i
            off_y = (spot // side - home_y + side) % side
            off_x = (spot % side - home_x + side) % side
            found.append(off_y * side + off_x if first_axis == "x" else off_x * side + off_y)
        return found

    def fill(number, slot):
        key_block = jnp.concatenate([keys[i] for i in slots_of(number)], axis=0)
        for cut in cuts:
            scores = jnp.dot(key_block, qs[:, cut], preferred_element_type=jnp.float32)
            scores = scores * scale + bias[...]
            sbuf[slot, :, cut] = scores
            mbuf[slot, :, cut] = jnp.max(scores, axis=0, keepdims=True)

    def use(number, slot):
        shift = slope_two * (number * rows - last_query).astype(jnp.float32)
        value_block = jnp.concatenate([values[i] for i in slots_of(number)], axis=1)
        value_block = jnp.concatenate([value_block, jnp.ones((16, rows), jnp.bfloat16)], axis=0)
        for cut in cuts:
            old = top[:, cut]
            new = jnp.maximum(old, mbuf[slot, :, cut] + shift)
            probs = jnp.exp2(sbuf[slot, :, cut] - (new - shift)).astype(jnp.bfloat16)
            top[:, cut] = new
            product = jnp.dot(value_block, probs, preferred_element_type=jnp.float32)
            acc[:, cut] = acc[:, cut] * jnp.exp2(old - new) + product

    def hide_later_keys(number, slot):
        for cut in cuts:
            lane = lax.broadcasted_iota(jnp.int32, (rows, LANES), 1) + cut.start
            lane = jnp.where(lane >= chunk, lane - chunk, lane)
            key_place = lax.broadcasted_iota(jnp.int32, (rows, LANES), 0) + number * rows
            scores = jnp.where(key_place <= lane + place * chunk, sbuf[slot, :, cut], masked_score)
            sbuf[slot, :, cut] = scores
            mbuf[slot, :, cut] = jnp.max(scores, axis=0, keepdims=True)

    most = place_count // SPAN
    count = jnp.where(block > plane, most, jnp.where(block == plane, place // SPAN + 1, 0))

    @pl.when(count > 0)
    def _():
        fill(0, 0)
        last = count - 1

        def pair_step(pair, carry):
            fill(2 * pair + 1, 1)
            use(2 * pair, 0)
            fill(jnp.minimum(2 * pair + 2, most - 1), 0)
            use(2 * pair + 1, 1)
            return carry

        lax.fori_loop(0, last // 2, pair_step, 0)

        @pl.when(last % 2 == 1)
        def _():
            fill(last, 1)
            use(last - 1, 0)

            @pl.when(block == plane)
            def _():
                hide_later_keys(last, 1)

            use(last, 1)

        @pl.when(last % 2 == 0)
        def _():
            @pl.when(block == plane)
            def _():
                hide_later_keys(last, 0)

            use(last, 0)

    sums = jnp.maximum(acc[vsize : vsize + 1, :], 1e-30)
    mixed = acc[:vsize, :] * (1.0 / sums)
    level = top[...] + jnp.log2(sums)
    lam_row = jnp.full((1, chunk), lam[0], jnp.float32)
    start = 2 * vsize * number
    for j in range(2):
        column = start + j * vsize
        out[0, :, column : column + vsize] = (
            mixed[:, j * chunk : (j + 1) * chunk].T.astype(jnp.bfloat16)
        )
        for k, part in enumerate(three_parts(level[:, j * chunk : (j + 1) * chunk])):
            row = 6 * k + 2 * number + j
            tail[row : row + 1, :] = part
    for k, part in enumerate(three_parts(lam_row)):
        row = 6 * k + 4 + number
        tail[row : row + 1, :] = part
    tails = tail[...].T
    if number:
        out[0, :, :start] = prior[0, :, :start]
        tails = tails + prior[0, :, start:].astype(jnp.float32)
    out[0, :, start + 2 * vsize :] = tails.astype(jnp.bfloat16)


def flash(number, meta, slope, lam, queries, pieces, prior, first_axis):
    blocks, _, chunk = queries.shape
    vsize = 128
    width = pieces[0].shape[2] - vsize
    place_count = sum(piece.shape[0] for piece in pieces)
    rows = SPAN * chunk
    q_row = 0 if number else 2
    lanes_out = 2 * vsize * (number + 1) + vsize
    scalar = pl.BlockSpec(memory_space=pltpu.SMEM)

    def own_block(b, meta):
        return ((meta[1] + b) % blocks, 0, 0)

    specs = [scalar, scalar, pl.BlockSpec((1, width, chunk), lambda b, meta: (b, q_row, 0))]
    specs += [pl.BlockSpec(piece.shape, lambda b, meta: (0, 0, 0)) for piece in pieces]
    operands = [slope, lam, queries, *pieces]
    if number:
        specs.append(pl.BlockSpec((1, chunk, prior.shape[2]), own_block))
        operands.append(prior)
    return pl.pallas_call(
        lambda *refs: flash_body(*refs, first_axis=first_axis, number=number),
        grid_spec=pltpu.PrefetchScalarGridSpec(
            num_scalar_prefetch=1,
            grid=(blocks,),
            in_specs=specs,
            out_specs=pl.BlockSpec((1, chunk, lanes_out), own_block),
            scratch_shapes=[
                pltpu.VMEM((place_count, chunk, width), jnp.bfloat16),
                pltpu.VMEM((place_count, vsize, chunk), jnp.bfloat16),
                pltpu.VMEM((width, 2 * chunk), jnp.bfloat16),
                pltpu.VMEM((rows, LANES), jnp.float32),
                pltpu.VMEM((1, 2 * chunk), jnp.float32),
                pltpu.VMEM((vsize + 16, 2 * chunk), jnp.float32),
                pltpu.VMEM((2, rows, 2 * chunk), jnp.float32),
                pltpu.VMEM((2, 1, 2 * chunk), jnp.float32),
                pltpu.VMEM((vsize, chunk), jnp.float32),
            ],
        ),
        out_shape=jax.ShapeDtypeStruct((blocks, chunk, lanes_out), jnp.bfloat16),
        cost_estimate=pl.CostEstimate(flops=20_000_000_000, transcendentals=0, bytes_accessed=0),
        compiler_params=pltpu.CompilerParams(
            dimension_semantics=("arbitrary",), vmem_limit_bytes=VMEM_LIMIT
        ),
    )(meta, *operands)


def around(value, axis):
    size = lax.axis_size(axis)
    cut = value.shape[0] // 2
    ahead = [((i + 1) % size, i) for i in range(size)]
    behind = [((i - 1) % size, i) for i in range(size)]
    one = lax.ppermute(value, axis, ahead)
    three = lax.ppermute(value, axis, behind)
    two_first = lax.ppermute(one[:cut], axis, ahead)
    two_last = lax.ppermute(three[cut:], axis, behind)
    return [value, one, two_first, two_last, three]


def normed(values, gain_row):
    average = jnp.mean(values, axis=-1, keepdims=True)
    centred = values - average
    variance = jnp.mean(centred * centred, axis=-1, keepdims=True)
    return centred * lax.rsqrt(variance + epsilon) * gain_row


def merge_body(core, arrived, head_gain, residual, weight, norm_gain, middle, keep, give):
    planes = arrived.shape[0] // 2
    vsize = head_gain.shape[1]
    gain = head_gain[...].astype(jnp.float32)
    pieces = []
    for head in range(2):
        tails = []
        for z in range(planes):
            lanes = arrived[2 * z + head, :, 4 * vsize :].astype(jnp.float32)
            tails.append([lanes[:, i : i + 1] + lanes[:, i + 6 : i + 7] + lanes[:, i + 12 : i + 13] for i in range(6)])
        for group in range(2):
            mixtures = []
            for j in range(2):
                index = 2 * group + j
                highest = tails[0][index]
                for z in range(1, planes):
                    highest = jnp.maximum(highest, tails[z][index])
                weights = [jnp.exp2(tails[z][index] - highest) for z in range(planes)]
                scaled = 1.0 / sum(weights)
                column = index * vsize
                mixtures.append(
                    sum(
                        (weights[z] * scaled)
                        * arrived[2 * z + head, :, column : column + vsize].astype(jnp.float32)
                        for z in range(planes)
                    )
                )
            head_out = mixtures[0] - tails[0][4 + group] * mixtures[1]
            power = jnp.mean(head_out * head_out, axis=-1, keepdims=True)
            pieces.append((head_out * lax.rsqrt(power + epsilon) * gain).astype(jnp.bfloat16))
    attended = jnp.concatenate(pieces, axis=1)
    projected = jnp.dot(attended, weight[...], preferred_element_type=jnp.float32)
    values = residual_gain * residual[...].astype(jnp.float32) + projected
    result = normed(values, norm_gain[...].astype(jnp.float32)).astype(jnp.bfloat16)
    middle[...] = result
    half = result.shape[1] // 2

    @pl.when(core[0] == 0)
    def _():
        keep[...] = result[:, :half]
        give[...] = result[:, half:]

    @pl.when(core[0] == 1)
    def _():
        keep[...] = result[:, half:]
        give[...] = result[:, :half]


def merge(core, arrived, head_gain, residual, weight, norm_gain):
    count, features = residual.shape
    return pl.pallas_call(
        merge_body,
        in_specs=[pl.BlockSpec(memory_space=pltpu.SMEM)] + [pl.BlockSpec(memory_space=pltpu.VMEM)] * 5,
        out_shape=[
            jax.ShapeDtypeStruct((count, features), jnp.bfloat16),
            jax.ShapeDtypeStruct((count, features // 2), jnp.bfloat16),
            jax.ShapeDtypeStruct((count, features // 2), jnp.bfloat16),
        ],
        cost_estimate=pl.CostEstimate(flops=5_000_000_000, transcendentals=0, bytes_accessed=0),
        compiler_params=pltpu.CompilerParams(vmem_limit_bytes=VMEM_LIMIT),
    )(core, arrived, head_gain, residual, weight, norm_gain)


def expert_body(core, mine, other, gate, up, down, keep, give):
    half = mine.shape[1]
    first = pl.multiple_of(core[0] * half, half)
    second = pl.multiple_of((1 - core[0]) * half, half)
    own_rows = mine[...]
    other_rows = other[...]

    def through(weight):
        return jnp.dot(
            own_rows, weight[0, pl.ds(first, half), :], preferred_element_type=jnp.float32
        ) + jnp.dot(
            other_rows, weight[0, pl.ds(second, half), :], preferred_element_type=jnp.float32
        )

    gate_in = through(gate)
    upward = through(up)
    hidden = (gate_in * (1.0 / (1.0 + jnp.exp(-gate_in))) * upward).astype(jnp.bfloat16)
    keep[...] = jnp.dot(
        hidden, down[0, :, pl.ds(first, half)], preferred_element_type=jnp.float32
    ).astype(jnp.bfloat16)
    give[...] = jnp.dot(
        hidden, down[0, :, pl.ds(second, half)], preferred_element_type=jnp.float32
    ).astype(jnp.bfloat16)


def expert(core, mine, other, gate, up, down):
    count, half = mine.shape
    block_rows = 256
    rows = pl.BlockSpec((block_rows, half), lambda i: (i, 0))
    shape = jax.ShapeDtypeStruct((count, half), jnp.bfloat16)
    return pl.pallas_call(
        expert_body,
        grid=(count // block_rows,),
        in_specs=[
            pl.BlockSpec(memory_space=pltpu.SMEM),
            rows,
            rows,
            pl.BlockSpec(gate.shape, lambda i: (0, 0, 0)),
            pl.BlockSpec(up.shape, lambda i: (0, 0, 0)),
            pl.BlockSpec(down.shape, lambda i: (0, 0, 0)),
        ],
        out_specs=[rows, rows],
        out_shape=[shape, shape],
        cost_estimate=pl.CostEstimate(flops=count * 12_000_000, transcendentals=0, bytes_accessed=0),
        compiler_params=pltpu.CompilerParams(
            dimension_semantics=("arbitrary",), vmem_limit_bytes=VMEM_LIMIT
        ),
    )(core, mine, other, gate, up, down)


def final_body(core, own, received, middle, norm_gain, out, total):
    half = own.shape[1]

    @pl.when(core[0] == 0)
    def _():
        total[:, :half] = own[...]
        total[:, half:] = received[...]

    @pl.when(core[0] == 1)
    def _():
        total[:, :half] = received[...]
        total[:, half:] = own[...]

    values = residual_gain * middle[...].astype(jnp.float32) + total[...]
    out[...] = normed(values, norm_gain[...].astype(jnp.float32)).astype(jnp.bfloat16)


def final(core, own, received, middle, norm_gain):
    return pl.pallas_call(
        final_body,
        in_specs=[pl.BlockSpec(memory_space=pltpu.SMEM)] + [pl.BlockSpec(memory_space=pltpu.VMEM)] * 4,
        out_shape=jax.ShapeDtypeStruct(middle.shape, jnp.bfloat16),
        scratch_shapes=[pltpu.VMEM(middle.shape, jnp.float32)],
        cost_estimate=pl.CostEstimate(flops=2_000_000_000, transcendentals=0, bytes_accessed=0),
        compiler_params=pltpu.CompilerParams(vmem_limit_bytes=VMEM_LIMIT),
    )(core, own, received, middle, norm_gain)


def slots(routes, experts, offset):
    chosen = routes.reshape(-1)
    matches = (chosen[:, None] == jnp.arange(experts)[None, :]).astype(jnp.int32)
    earlier = jnp.cumsum(matches, axis=0) - matches
    rank = jnp.sum(earlier * matches, axis=1)
    return routes, (offset + rank).reshape(routes.shape)


def shards(
    query_small,
    key_small,
    value_small,
    query_large,
    key_large,
    value_large,
    lambdas,
    slopes,
    head_gain,
    residual,
    out_weight,
    norm_gains,
    routes,
    route_weights,
    gate_weight,
    up_weight,
    down_weight,
):
    length = query_small.shape[0]
    planes = lax.axis_size("z")
    plane = lax.axis_index("z")
    core = lax.axis_index("tp")
    mirror = [(i, planes - 1 - i) for i in range(planes)]
    swap = [(0, 1), (1, 0)]
    small_pack = jnp.concatenate(
        [key_small.reshape(length, -1), value_small.reshape(length, -1)], axis=1
    )
    large_pack = jnp.concatenate(
        [key_large.reshape(length, -1), value_large.reshape(length, -1)], axis=1
    )
    query_pack = jnp.concatenate(
        [query_large.reshape(length, -1).T, query_small.reshape(length, -1).T], axis=0
    )
    small_pack = lax.ppermute(small_pack, "z", mirror)
    queries = jnp.concatenate(around(query_pack, "z"), axis=0).reshape(planes, *query_pack.shape)
    large_row = jnp.concatenate(around(large_pack, "x"), axis=0).reshape(4, *large_pack.shape)
    small_row = jnp.concatenate(around(small_pack, "y"), axis=0).reshape(4, *small_pack.shape)
    large_row, small_row, queries = lax.optimization_barrier((large_row, small_row, queries))
    small_pieces = around(small_row, "x")
    large_pieces = around(large_row, "y")

    core_count = lax.axis_size("tp")
    row_count = length // core_count
    experts = lax.axis_size(SP)
    block = core_count * (4 * row_count // experts)
    their_routes = lax.ppermute(routes, "tp", swap)
    their_weights = lax.ppermute(route_weights, "tp", swap)
    capacity = block // core_count
    tickets = [
        slots(routes, experts, core * capacity),
        slots(their_routes, experts, (1 - core) * capacity),
    ]
    chosen = jnp.concatenate([tickets[0][0], tickets[1][0]], axis=0)
    spot = jnp.concatenate([tickets[0][1], tickets[1][1]], axis=0)
    shares = jnp.concatenate([route_weights, their_weights], axis=0)
    cuts = ((0, 16), (16, 8))
    selectors = []
    spreads = []
    for first, width in cuts:
        row = jnp.where((spot >= first) & (spot < first + width), chosen * width + spot - first, -1)
        places = jnp.arange(experts * width)
        selectors.append(
            ((row[:, 0][None, :] == places[:, None]) | (row[:, 1][None, :] == places[:, None])).astype(
                jnp.bfloat16
            )
        )
        spread = jnp.where(row[:, 0][:, None] == places[None, :], shares[:, :1], 0.0) + jnp.where(
            row[:, 1][:, None] == places[None, :], shares[:, 1:], 0.0
        )
        spread_top = lax.reduce_precision(spread, exponent_bits=8, mantissa_bits=7)
        spreads.append((spread_top.astype(jnp.bfloat16), (spread - spread_top).astype(jnp.bfloat16)))

    home = [plane, lax.axis_index("y"), lax.axis_index("x")]
    small_meta = jnp.stack([planes - 1 - plane, *home]).astype(jnp.int32)
    large_meta = jnp.stack([plane, *home]).astype(jnp.int32)
    parts = flash(
        0, small_meta, slopes[0, :1], lambdas[0, :1], queries, small_pieces, None, "y"
    )
    parts = flash(
        1, large_meta, slopes[0, 1:], lambdas[0, 1:], queries, large_pieces, parts, "x"
    )
    parts = parts.reshape(planes * core_count, row_count, -1)
    parts = lax.all_to_all(parts, OWNERS, split_axis=0, concat_axis=0, tiled=True)
    which = core.astype(jnp.int32).reshape(1)
    middle, keep, give = merge(
        which, parts, head_gain.reshape(1, -1), residual, out_weight, norm_gains[:1]
    )
    half = keep.shape[1]
    tokens = jnp.concatenate([keep, lax.ppermute(give, "tp", swap)], axis=0)
    arrived = []
    for (first, width), selector in zip(cuts, selectors):
        outgoing = jnp.dot(selector, tokens, preferred_element_type=jnp.float32).astype(jnp.bfloat16)
        came = lax.all_to_all(
            outgoing.reshape(experts, width, half), SP, split_axis=0, concat_axis=0, tiled=True
        )
        arrived.append(came.reshape(experts * width, half))
    returned = []
    for (first, width), mine in zip(cuts, arrived):
        other = lax.ppermute(mine, "tp", swap)
        kept, given = expert(which, mine, other, gate_weight, up_weight, down_weight)
        got = lax.ppermute(given, "tp", swap)
        summed = (kept.astype(jnp.float32) + got.astype(jnp.float32)).astype(jnp.bfloat16)
        came = lax.all_to_all(
            summed.reshape(experts, width, half), SP, split_axis=0, concat_axis=0, tiled=True
        )
        returned.append(came.reshape(experts * width, half))

    def weighed(first):
        cut = slice(first, first + row_count)
        return sum(
            jnp.dot(high[cut], rows, preferred_element_type=jnp.float32)
            + jnp.dot(low[cut], rows, preferred_element_type=jnp.float32)
            for (high, low), rows in zip(spreads, returned)
        )

    received = lax.ppermute(weighed(row_count), "tp", swap)
    return final(which, weighed(0), received, middle, norm_gains[1:])


def solution(mesh):
    cube = Mesh(mesh.devices.reshape(4, 4, 4, 2), ("z", "y", "x", "tp"))
    both = SP + ("tp",)
    placed = (
        P(SP, "tp", None),
        P(SP, "tp", None),
        P(SP, "tp", None),
        P(SP, "tp", None),
        P(SP, "tp", None),
        P(SP, "tp", None),
        P("tp", None),
        P("tp", None),
        P(),
        P(both, None),
        P(),
        P(),
        P(both, None),
        P(both, None),
        P(SP, None, "tp"),
        P(SP, None, "tp"),
        P(SP, "tp", None),
    )

    return jax.shard_map(
        shards, mesh=cube, in_specs=placed, out_specs=P(both, None), check_vma=False
    )
```

```python
import jax
import jax.numpy as jnp
from jax import lax
from jax.experimental import pallas as pl
from jax.experimental.pallas import tpu as pltpu
from jax.sharding import Mesh, PartitionSpec as P

residual_gain = 8.0**0.25
epsilon = 1e-05
masked_score = -1e30
LOG2E = 1.4426950408889634
SP = ("z", "y", "x")
OWNERS = ("z", "tp")
SPAN = 2
LANES = 256
VMEM_LIMIT = 56 * 1024 * 1024


def three_parts(value):
    high = value.astype(jnp.bfloat16).astype(jnp.float32)
    rest = value - high
    middle = rest.astype(jnp.bfloat16).astype(jnp.float32)
    return high, middle, (rest - middle).astype(jnp.bfloat16).astype(jnp.float32)


def flash_body(meta, slope, lam, qt, *refs, first_axis, number):
    pieces, rest = refs[:8], refs[8:]
    prior = rest[0] if number else None
    out, keys, values, qs, bias, top, acc, sbuf, mbuf, tail = rest[number:]
    chunk, vsize = qt.shape[2], values.shape[1]
    width = qt.shape[1]
    half = width // 2
    place_count = keys.shape[0]
    side = 4
    plane, home_y, home_x = meta[0], meta[2], meta[3]
    place = home_y * side + home_x
    block = (meta[1] + pl.program_id(0)) % side
    scale = LOG2E * half ** (-0.5)
    slope_two = slope[0] * LOG2E
    rows = SPAN * chunk
    total = 2 * chunk

    @pl.when(pl.program_id(0) == 0)
    def _():
        slot = 0
        for piece in pieces:
            for i in range(piece.shape[0]):
                keys[slot] = piece[i, :, :width]
                values[slot] = piece[i, :, width:].T
                slot += 1

    qs[...] = jnp.zeros_like(qs)
    qs[:half, :chunk] = qt[0, :half, :]
    qs[half:, chunk:] = qt[0, half:, :]
    bias[...] = slope_two * lax.broadcasted_iota(jnp.int32, bias.shape, 0).astype(jnp.float32)
    top[...] = jnp.full_like(top, masked_score)
    acc[...] = jnp.zeros_like(acc)
    tail[...] = jnp.zeros_like(tail)
    last_query = (block - plane) * (place_count * chunk) + place * chunk + (chunk - 1)
    cuts = [slice(first, first + LANES) for first in range(0, total, LANES)]

    def slots_of(number):
        found = []
        for i in range(SPAN):
            spot = number * SPAN + i
            off_y = (spot // side - home_y + side) % side
            off_x = (spot % side - home_x + side) % side
            found.append(off_y * side + off_x if first_axis == "x" else off_x * side + off_y)
        return found

    def fill(number, slot):
        key_block = jnp.concatenate([keys[i] for i in slots_of(number)], axis=0)
        for cut in cuts:
            scores = jnp.dot(key_block, qs[:, cut], preferred_element_type=jnp.float32)
            scores = scores * scale + bias[...]
            sbuf[slot, :, cut] = scores
            mbuf[slot, :, cut] = jnp.max(scores, axis=0, keepdims=True)

    def use(number, slot):
        shift = slope_two * (number * rows - last_query).astype(jnp.float32)
        value_block = jnp.concatenate([values[i] for i in slots_of(number)], axis=1)
        value_block = jnp.concatenate([value_block, jnp.ones((16, rows), jnp.bfloat16)], axis=0)
        for cut in cuts:
            old = top[:, cut]
            new = jnp.maximum(old, mbuf[slot, :, cut] + shift)
            probs = jnp.exp2(sbuf[slot, :, cut] - (new - shift)).astype(jnp.bfloat16)
            top[:, cut] = new
            product = jnp.dot(value_block, probs, preferred_element_type=jnp.float32)
            acc[:, cut] = acc[:, cut] * jnp.exp2(old - new) + product

    def hide_later_keys(number, slot):
        for cut in cuts:
            lane = lax.broadcasted_iota(jnp.int32, (rows, LANES), 1) + cut.start
            lane = jnp.where(lane >= chunk, lane - chunk, lane)
            key_place = lax.broadcasted_iota(jnp.int32, (rows, LANES), 0) + number * rows
            scores = jnp.where(key_place <= lane + place * chunk, sbuf[slot, :, cut], masked_score)
            sbuf[slot, :, cut] = scores
            mbuf[slot, :, cut] = jnp.max(scores, axis=0, keepdims=True)

    most = place_count // SPAN
    count = jnp.where(block > plane, most, jnp.where(block == plane, place // SPAN + 1, 0))

    @pl.when(count > 0)
    def _():
        fill(0, 0)
        last = count - 1

        def pair_step(pair, carry):
            fill(2 * pair + 1, 1)
            use(2 * pair, 0)
            fill(jnp.minimum(2 * pair + 2, most - 1), 0)
            use(2 * pair + 1, 1)
            return carry

        lax.fori_loop(0, last // 2, pair_step, 0)

        @pl.when(last % 2 == 1)
        def _():
            fill(last, 1)
            use(last - 1, 0)

            @pl.when(block == plane)
            def _():
                hide_later_keys(last, 1)

            use(last, 1)

        @pl.when(last % 2 == 0)
        def _():
            @pl.when(block == plane)
            def _():
                hide_later_keys(last, 0)

            use(last, 0)

    sums = jnp.maximum(acc[vsize : vsize + 1, :], 1e-30)
    mixed = acc[:vsize, :] * (1.0 / sums)
    level = top[...] + jnp.log2(sums)
    lam_row = jnp.full((1, chunk), lam[0], jnp.float32)
    start = 2 * vsize * number
    for j in range(2):
        column = start + j * vsize
        out[0, :, column : column + vsize] = (
            mixed[:, j * chunk : (j + 1) * chunk].T.astype(jnp.bfloat16)
        )
        for k, part in enumerate(three_parts(level[:, j * chunk : (j + 1) * chunk])):
            row = 6 * k + 2 * number + j
            tail[row : row + 1, :] = part
    for k, part in enumerate(three_parts(lam_row)):
        row = 6 * k + 4 + number
        tail[row : row + 1, :] = part
    tails = tail[...].T
    if number:
        out[0, :, :start] = prior[0, :, :start]
        tails = tails + prior[0, :, start:].astype(jnp.float32)
    out[0, :, start + 2 * vsize :] = tails.astype(jnp.bfloat16)


def flash(number, meta, slope, lam, queries, pieces, prior, first_axis):
    blocks, _, chunk = queries.shape
    vsize = 128
    width = pieces[0].shape[2] - vsize
    place_count = sum(piece.shape[0] for piece in pieces)
    rows = SPAN * chunk
    q_row = 0 if number else 2
    lanes_out = 2 * vsize * (number + 1) + vsize
    scalar = pl.BlockSpec(memory_space=pltpu.SMEM)

    def own_block(b, meta):
        return ((meta[1] + b) % blocks, 0, 0)

    specs = [scalar, scalar, pl.BlockSpec((1, width, chunk), lambda b, meta: (b, q_row, 0))]
    specs += [pl.BlockSpec(piece.shape, lambda b, meta: (0, 0, 0)) for piece in pieces]
    operands = [slope, lam, queries, *pieces]
    if number:
        specs.append(pl.BlockSpec((1, chunk, prior.shape[2]), own_block))
        operands.append(prior)
    return pl.pallas_call(
        lambda *refs: flash_body(*refs, first_axis=first_axis, number=number),
        grid_spec=pltpu.PrefetchScalarGridSpec(
            num_scalar_prefetch=1,
            grid=(blocks,),
            in_specs=specs,
            out_specs=pl.BlockSpec((1, chunk, lanes_out), own_block),
            scratch_shapes=[
                pltpu.VMEM((place_count, chunk, width), jnp.bfloat16),
                pltpu.VMEM((place_count, vsize, chunk), jnp.bfloat16),
                pltpu.VMEM((width, 2 * chunk), jnp.bfloat16),
                pltpu.VMEM((rows, LANES), jnp.float32),
                pltpu.VMEM((1, 2 * chunk), jnp.float32),
                pltpu.VMEM((vsize + 16, 2 * chunk), jnp.float32),
                pltpu.VMEM((2, rows, 2 * chunk), jnp.float32),
                pltpu.VMEM((2, 1, 2 * chunk), jnp.float32),
                pltpu.VMEM((vsize, chunk), jnp.float32),
            ],
        ),
        out_shape=jax.ShapeDtypeStruct((blocks, chunk, lanes_out), jnp.bfloat16),
        cost_estimate=pl.CostEstimate(flops=20_000_000_000, transcendentals=0, bytes_accessed=0),
        compiler_params=pltpu.CompilerParams(
            dimension_semantics=("arbitrary",), vmem_limit_bytes=VMEM_LIMIT
        ),
    )(meta, *operands)


def neighbours(size):
    ahead = [((i + 1) % size, i) for i in range(size)]
    behind = [((i - 1) % size, i) for i in range(size)]
    return ahead, behind


def passed_on(value, one, three, axis):
    ahead, behind = neighbours(lax.axis_size(axis))
    cut = value.shape[0] // 2
    two_first = lax.ppermute(one[:cut], axis, ahead)
    two_last = lax.ppermute(three[cut:], axis, behind)
    return [value, one, two_first, two_last, three]


def first_sends(value, axis):
    ahead, behind = neighbours(lax.axis_size(axis))
    return value, lax.ppermute(value, axis, ahead), lax.ppermute(value, axis, behind)


def mirrored_sends(value, axis):
    planes, size = lax.axis_size("z"), lax.axis_size(axis)

    def send(step):
        pairs = [
            ((planes - 1 - z) * size + (i + step) % size, z * size + i)
            for z in range(planes)
            for i in range(size)
        ]
        return lax.ppermute(value, ("z", axis), pairs)

    return send(0), send(1), send(-1)


def stack_body(*refs):
    for outs, pieces in ((refs[10:12], refs[:5]), (refs[12:14], refs[5:10])):
        cut = pieces[2].shape[0]
        outs[0][0] = pieces[0][...]
        outs[0][1] = pieces[1][...]
        outs[1][0, :cut] = pieces[2][...]
        outs[1][0, cut:] = pieces[3][...]
        outs[1][1] = pieces[4][...]


def stacked(first, second):
    shapes = [jax.ShapeDtypeStruct((2, *pieces[0].shape), jnp.bfloat16) for pieces in (first, second)]
    return pl.pallas_call(
        stack_body,
        in_specs=[pl.BlockSpec(memory_space=pltpu.VMEM)] * 10,
        out_shape=[shapes[0], shapes[0], shapes[1], shapes[1]],
        compiler_params=pltpu.CompilerParams(vmem_limit_bytes=VMEM_LIMIT),
    )(*first, *second)


def around_in_halves(front, back, axis):
    ahead, behind = neighbours(lax.axis_size(axis))
    one_front = lax.ppermute(front, axis, ahead)
    three_back = lax.ppermute(back, axis, behind)
    one_back = lax.ppermute(back, axis, ahead)
    three_front = lax.ppermute(front, axis, behind)
    two_front = lax.ppermute(one_front, axis, ahead)
    two_back = lax.ppermute(three_back, axis, behind)
    return [front, back, one_front, one_back, two_front, two_back, three_front, three_back]


def normed(values, gain_row):
    average = jnp.mean(values, axis=-1, keepdims=True)
    centred = values - average
    variance = jnp.mean(centred * centred, axis=-1, keepdims=True)
    return centred * lax.rsqrt(variance + epsilon) * gain_row


def merge_body(core, arrived, head_gain, residual, weight, norm_gain, middle, keep, give):
    planes = arrived.shape[0] // 2
    vsize = head_gain.shape[1]
    gain = head_gain[...].astype(jnp.float32)
    pieces = []
    for head in range(2):
        tails = []
        for z in range(planes):
            lanes = arrived[2 * z + head, :, 4 * vsize :].astype(jnp.float32)
            tails.append([lanes[:, i : i + 1] + lanes[:, i + 6 : i + 7] + lanes[:, i + 12 : i + 13] for i in range(6)])
        for group in range(2):
            mixtures = []
            for j in range(2):
                index = 2 * group + j
                highest = tails[0][index]
                for z in range(1, planes):
                    highest = jnp.maximum(highest, tails[z][index])
                weights = [jnp.exp2(tails[z][index] - highest) for z in range(planes)]
                scaled = 1.0 / sum(weights)
                column = index * vsize
                mixtures.append(
                    sum(
                        (weights[z] * scaled)
                        * arrived[2 * z + head, :, column : column + vsize].astype(jnp.float32)
                        for z in range(planes)
                    )
                )
            head_out = mixtures[0] - tails[0][4 + group] * mixtures[1]
            power = jnp.mean(head_out * head_out, axis=-1, keepdims=True)
            pieces.append((head_out * lax.rsqrt(power + epsilon) * gain).astype(jnp.bfloat16))
    attended = jnp.concatenate(pieces, axis=1)
    projected = jnp.dot(attended, weight[...], preferred_element_type=jnp.float32)
    values = residual_gain * residual[...].astype(jnp.float32) + projected
    result = normed(values, norm_gain[...].astype(jnp.float32)).astype(jnp.bfloat16)
    middle[...] = result
    half = result.shape[1] // 2

    @pl.when(core[0] == 0)
    def _():
        keep[...] = result[:, :half]
        give[...] = result[:, half:]

    @pl.when(core[0] == 1)
    def _():
        keep[...] = result[:, half:]
        give[...] = result[:, :half]


def merge(core, arrived, head_gain, residual, weight, norm_gain):
    count, features = residual.shape
    return pl.pallas_call(
        merge_body,
        in_specs=[pl.BlockSpec(memory_space=pltpu.SMEM)] + [pl.BlockSpec(memory_space=pltpu.VMEM)] * 5,
        out_shape=[
            jax.ShapeDtypeStruct((count, features), jnp.bfloat16),
            jax.ShapeDtypeStruct((count, features // 2), jnp.bfloat16),
            jax.ShapeDtypeStruct((count, features // 2), jnp.bfloat16),
        ],
        cost_estimate=pl.CostEstimate(flops=5_000_000_000, transcendentals=0, bytes_accessed=0),
        compiler_params=pltpu.CompilerParams(vmem_limit_bytes=VMEM_LIMIT),
    )(core, arrived, head_gain, residual, weight, norm_gain)


def expert_body(core, mine, other, gate, up, down, keep, give):
    half = mine.shape[1]
    first = pl.multiple_of(core[0] * half, half)
    second = pl.multiple_of((1 - core[0]) * half, half)
    own_rows = mine[...]
    other_rows = other[...]

    def through(weight):
        return jnp.dot(
            own_rows, weight[0, pl.ds(first, half), :], preferred_element_type=jnp.float32
        ) + jnp.dot(
            other_rows, weight[0, pl.ds(second, half), :], preferred_element_type=jnp.float32
        )

    gate_in = through(gate)
    upward = through(up)
    hidden = (gate_in * (1.0 / (1.0 + jnp.exp(-gate_in))) * upward).astype(jnp.bfloat16)
    keep[...] = jnp.dot(
        hidden, down[0, :, pl.ds(first, half)], preferred_element_type=jnp.float32
    ).astype(jnp.bfloat16)
    give[...] = jnp.dot(
        hidden, down[0, :, pl.ds(second, half)], preferred_element_type=jnp.float32
    ).astype(jnp.bfloat16)


def expert(core, mine, other, gate, up, down):
    count, half = mine.shape
    block_rows = 256
    rows = pl.BlockSpec((block_rows, half), lambda i: (i, 0))
    shape = jax.ShapeDtypeStruct((count, half), jnp.bfloat16)
    return pl.pallas_call(
        expert_body,
        grid=(count // block_rows,),
        in_specs=[
            pl.BlockSpec(memory_space=pltpu.SMEM),
            rows,
            rows,
            pl.BlockSpec(gate.shape, lambda i: (0, 0, 0)),
            pl.BlockSpec(up.shape, lambda i: (0, 0, 0)),
            pl.BlockSpec(down.shape, lambda i: (0, 0, 0)),
        ],
        out_specs=[rows, rows],
        out_shape=[shape, shape],
        cost_estimate=pl.CostEstimate(flops=count * 12_000_000, transcendentals=0, bytes_accessed=0),
        compiler_params=pltpu.CompilerParams(
            dimension_semantics=("arbitrary",), vmem_limit_bytes=VMEM_LIMIT
        ),
    )(core, mine, other, gate, up, down)


def final_body(core, own, received, middle, norm_gain, out, total):
    half = own.shape[1]

    @pl.when(core[0] == 0)
    def _():
        total[:, :half] = own[...]
        total[:, half:] = received[...]

    @pl.when(core[0] == 1)
    def _():
        total[:, :half] = received[...]
        total[:, half:] = own[...]

    values = residual_gain * middle[...].astype(jnp.float32) + total[...]
    out[...] = normed(values, norm_gain[...].astype(jnp.float32)).astype(jnp.bfloat16)


def final(core, own, received, middle, norm_gain):
    return pl.pallas_call(
        final_body,
        in_specs=[pl.BlockSpec(memory_space=pltpu.SMEM)] + [pl.BlockSpec(memory_space=pltpu.VMEM)] * 4,
        out_shape=jax.ShapeDtypeStruct(middle.shape, jnp.bfloat16),
        scratch_shapes=[pltpu.VMEM(middle.shape, jnp.float32)],
        cost_estimate=pl.CostEstimate(flops=2_000_000_000, transcendentals=0, bytes_accessed=0),
        compiler_params=pltpu.CompilerParams(vmem_limit_bytes=VMEM_LIMIT),
    )(core, own, received, middle, norm_gain)


def slots(routes, experts, offset):
    chosen = routes.reshape(-1)
    matches = (chosen[:, None] == jnp.arange(experts)[None, :]).astype(jnp.int32)
    earlier = jnp.cumsum(matches, axis=0) - matches
    rank = jnp.sum(earlier * matches, axis=1)
    return routes, (offset + rank).reshape(routes.shape)


def shards(
    query_small,
    key_small,
    value_small,
    query_large,
    key_large,
    value_large,
    lambdas,
    slopes,
    head_gain,
    residual,
    out_weight,
    norm_gains,
    routes,
    route_weights,
    gate_weight,
    up_weight,
    down_weight,
):
    length = query_small.shape[0]
    planes = lax.axis_size("z")
    plane = lax.axis_index("z")
    core = lax.axis_index("tp")
    swap = [(0, 1), (1, 0)]
    small_pack = jnp.concatenate(
        [key_small.reshape(length, -1), value_small.reshape(length, -1)], axis=1
    )
    large_pack = jnp.concatenate(
        [key_large.reshape(length, -1), value_large.reshape(length, -1)], axis=1
    )
    query_pack = jnp.concatenate(
        [query_large.reshape(length, -1).T, query_small.reshape(length, -1).T], axis=0
    )
    large_parts = passed_on(*first_sends(large_pack, "x"), "x")
    small_parts = passed_on(*mirrored_sends(small_pack, "y"), "y")
    rows = stacked(large_parts, small_parts)
    rows, query_pack = lax.optimization_barrier((rows, query_pack))
    query_sends = first_sends(query_pack, "z")
    large_pieces = around_in_halves(rows[0], rows[1], "y")
    small_pieces = around_in_halves(rows[2], rows[3], "x")
    queries = jnp.concatenate(passed_on(*query_sends, "z"), axis=0)
    queries = queries.reshape(planes, *query_pack.shape)

    core_count = lax.axis_size("tp")
    row_count = length // core_count
    experts = lax.axis_size(SP)
    block = core_count * (4 * row_count // experts)
    their_routes = lax.ppermute(routes, "tp", swap)
    their_weights = lax.ppermute(route_weights, "tp", swap)
    capacity = block // core_count
    tickets = [
        slots(routes, experts, core * capacity),
        slots(their_routes, experts, (1 - core) * capacity),
    ]
    chosen = jnp.concatenate([tickets[0][0], tickets[1][0]], axis=0)
    spot = jnp.concatenate([tickets[0][1], tickets[1][1]], axis=0)
    shares = jnp.concatenate([route_weights, their_weights], axis=0)
    cuts = ((0, 16), (16, 8))
    selectors = []
    spreads = []
    for first, width in cuts:
        row = jnp.where((spot >= first) & (spot < first + width), chosen * width + spot - first, -1)
        places = jnp.arange(experts * width)
        selectors.append(
            ((row[:, 0][None, :] == places[:, None]) | (row[:, 1][None, :] == places[:, None])).astype(
                jnp.bfloat16
            )
        )
        spread = jnp.where(row[:, 0][:, None] == places[None, :], shares[:, :1], 0.0) + jnp.where(
            row[:, 1][:, None] == places[None, :], shares[:, 1:], 0.0
        )
        spread_top = lax.reduce_precision(spread, exponent_bits=8, mantissa_bits=7)
        spreads.append((spread_top.astype(jnp.bfloat16), (spread - spread_top).astype(jnp.bfloat16)))

    home = [plane, lax.axis_index("y"), lax.axis_index("x")]
    small_meta = jnp.stack([planes - 1 - plane, *home]).astype(jnp.int32)
    large_meta = jnp.stack([plane, *home]).astype(jnp.int32)
    parts = flash(
        0, small_meta, slopes[0, :1], lambdas[0, :1], queries, small_pieces, None, "y"
    )
    parts = flash(
        1, large_meta, slopes[0, 1:], lambdas[0, 1:], queries, large_pieces, parts, "x"
    )
    parts = parts.reshape(planes * core_count, row_count, -1)
    parts = lax.all_to_all(parts, OWNERS, split_axis=0, concat_axis=0, tiled=True)
    which = core.astype(jnp.int32).reshape(1)
    middle, keep, give = merge(
        which, parts, head_gain.reshape(1, -1), residual, out_weight, norm_gains[:1]
    )
    half = keep.shape[1]
    tokens = jnp.concatenate([keep, lax.ppermute(give, "tp", swap)], axis=0)
    arrived = []
    for (first, width), selector in zip(cuts, selectors):
        outgoing = jnp.dot(selector, tokens, preferred_element_type=jnp.float32).astype(jnp.bfloat16)
        came = lax.all_to_all(
            outgoing.reshape(experts, width, half), SP, split_axis=0, concat_axis=0, tiled=True
        )
        arrived.append(came.reshape(experts * width, half))
    returned = []
    for (first, width), mine in zip(cuts, arrived):
        other = lax.ppermute(mine, "tp", swap)
        kept, given = expert(which, mine, other, gate_weight, up_weight, down_weight)
        got = lax.ppermute(given, "tp", swap)
        summed = (kept.astype(jnp.float32) + got.astype(jnp.float32)).astype(jnp.bfloat16)
        came = lax.all_to_all(
            summed.reshape(experts, width, half), SP, split_axis=0, concat_axis=0, tiled=True
        )
        returned.append(came.reshape(experts * width, half))

    def weighed(first):
        cut = slice(first, first + row_count)
        return sum(
            jnp.dot(high[cut], rows, preferred_element_type=jnp.float32)
            + jnp.dot(low[cut], rows, preferred_element_type=jnp.float32)
            for (high, low), rows in zip(spreads, returned)
        )

    received = lax.ppermute(weighed(row_count), "tp", swap)
    return final(which, weighed(0), received, middle, norm_gains[1:])


def solution(mesh):
    cube = Mesh(mesh.devices.reshape(4, 4, 4, 2), ("z", "y", "x", "tp"))
    both = SP + ("tp",)
    placed = (
        P(SP, "tp", None),
        P(SP, "tp", None),
        P(SP, "tp", None),
        P(SP, "tp", None),
        P(SP, "tp", None),
        P(SP, "tp", None),
        P("tp", None),
        P("tp", None),
        P(),
        P(both, None),
        P(),
        P(),
        P(both, None),
        P(both, None),
        P(SP, None, "tp"),
        P(SP, None, "tp"),
        P(SP, "tp", None),
    )

    return jax.shard_map(
        shards, mesh=cube, in_specs=placed, out_specs=P(both, None), check_vma=False
    )
```

```python
import jax
import jax.numpy as jnp
from jax import lax
from jax.experimental import pallas as pl
from jax.experimental.pallas import tpu as pltpu
from jax.sharding import Mesh, PartitionSpec as P

residual_gain = 8.0**0.25
epsilon = 1e-05
masked_score = -1e30
LOG2E = 1.4426950408889634
SP = ("z", "y", "x")
OWNERS = ("z", "tp")
SPAN = 4
LANES = 256
VMEM_LIMIT = 56 * 1024 * 1024


def three_parts(value):
    high = value.astype(jnp.bfloat16).astype(jnp.float32)
    rest = value - high
    middle = rest.astype(jnp.bfloat16).astype(jnp.float32)
    return high, middle, (rest - middle).astype(jnp.bfloat16).astype(jnp.float32)


def flash_body(meta, slope, lam, qt, *refs, first_axis, number):
    pieces, rest = refs[:8], refs[8:]
    prior = rest[0] if number else None
    out, keys, values, qs, bias, top, acc, sbuf, mbuf, tail = rest[number:]
    chunk, vsize = qt.shape[2], values.shape[1]
    width = qt.shape[1]
    half = width // 2
    place_count = keys.shape[0]
    side = 4
    plane, home_y, home_x = meta[0], meta[2], meta[3]
    place = home_y * side + home_x
    block = (meta[1] + pl.program_id(0)) % side
    scale = LOG2E * half ** (-0.5)
    slope_two = slope[0] * LOG2E
    rows = SPAN * chunk
    total = 2 * chunk

    @pl.when(pl.program_id(0) == 0)
    def _():
        slot = 0
        for piece in pieces:
            for i in range(piece.shape[0]):
                keys[slot] = piece[i, :, :width]
                values[slot] = piece[i, :, width:].T
                slot += 1

    qs[...] = jnp.zeros_like(qs)
    qs[:half, :chunk] = qt[0, :half, :]
    qs[half:, chunk:] = qt[0, half:, :]
    bias[...] = slope_two * lax.broadcasted_iota(jnp.int32, bias.shape, 0).astype(jnp.float32)
    top[...] = jnp.full_like(top, masked_score)
    acc[...] = jnp.zeros_like(acc)
    tail[...] = jnp.zeros_like(tail)
    last_query = (block - plane) * (place_count * chunk) + place * chunk + (chunk - 1)
    cuts = [slice(first, first + LANES) for first in range(0, total, LANES)]

    def slots_of(number):
        found = []
        for i in range(SPAN):
            spot = number * SPAN + i
            off_y = (spot // side - home_y + side) % side
            off_x = (spot % side - home_x + side) % side
            found.append(off_y * side + off_x if first_axis == "x" else off_x * side + off_y)
        return found

    def fill(number, slot):
        key_block = jnp.concatenate([keys[i] for i in slots_of(number)], axis=0)
        for cut in cuts:
            scores = jnp.dot(key_block, qs[:, cut], preferred_element_type=jnp.float32)
            scores = scores * scale + bias[...]
            sbuf[slot, :, cut] = scores
            mbuf[slot, :, cut] = jnp.max(scores, axis=0, keepdims=True)

    def use(number, slot):
        shift = slope_two * (number * rows - last_query).astype(jnp.float32)
        value_block = jnp.concatenate([values[i] for i in slots_of(number)], axis=1)
        value_block = jnp.concatenate([value_block, jnp.ones((16, rows), jnp.bfloat16)], axis=0)
        for cut in cuts:
            old = top[:, cut]
            new = jnp.maximum(old, mbuf[slot, :, cut] + shift)
            probs = jnp.exp2(sbuf[slot, :, cut] - (new - shift)).astype(jnp.bfloat16)
            top[:, cut] = new
            product = jnp.dot(value_block, probs, preferred_element_type=jnp.float32)
            acc[:, cut] = acc[:, cut] * jnp.exp2(old - new) + product

    def hide_later_keys(number, slot):
        for cut in cuts:
            lane = lax.broadcasted_iota(jnp.int32, (rows, LANES), 1) + cut.start
            lane = jnp.where(lane >= chunk, lane - chunk, lane)
            key_place = lax.broadcasted_iota(jnp.int32, (rows, LANES), 0) + number * rows
            scores = jnp.where(key_place <= lane + place * chunk, sbuf[slot, :, cut], masked_score)
            sbuf[slot, :, cut] = scores
            mbuf[slot, :, cut] = jnp.max(scores, axis=0, keepdims=True)

    most = place_count // SPAN
    count = jnp.where(block > plane, most, jnp.where(block == plane, place // SPAN + 1, 0))

    @pl.when(count > 0)
    def _():
        fill(0, 0)
        last = count - 1

        def pair_step(pair, carry):
            fill(2 * pair + 1, 1)
            use(2 * pair, 0)
            fill(jnp.minimum(2 * pair + 2, most - 1), 0)
            use(2 * pair + 1, 1)
            return carry

        lax.fori_loop(0, last // 2, pair_step, 0)

        @pl.when(last % 2 == 1)
        def _():
            fill(last, 1)
            use(last - 1, 0)

        @pl.when(block == plane)
        def _():
            hide_later_keys(last, last % 2)

        use(last, last % 2)

    sums = jnp.maximum(acc[vsize : vsize + 1, :], 1e-30)
    mixed = acc[:vsize, :] * (1.0 / sums)
    level = top[...] + jnp.log2(sums)
    lam_row = jnp.full((1, chunk), lam[0], jnp.float32)
    start = 2 * vsize * number
    for j in range(2):
        column = start + j * vsize
        out[0, :, column : column + vsize] = (
            mixed[:, j * chunk : (j + 1) * chunk].T.astype(jnp.bfloat16)
        )
        for k, part in enumerate(three_parts(level[:, j * chunk : (j + 1) * chunk])):
            row = 6 * k + 2 * number + j
            tail[row : row + 1, :] = part
    for k, part in enumerate(three_parts(lam_row)):
        row = 6 * k + 4 + number
        tail[row : row + 1, :] = part
    tails = tail[...].T
    if number:
        out[0, :, :start] = prior[0, :, :start]
        tails = tails + prior[0, :, start:].astype(jnp.float32)
    out[0, :, start + 2 * vsize :] = tails.astype(jnp.bfloat16)


def flash(number, meta, slope, lam, queries, pieces, prior, first_axis):
    blocks, _, chunk = queries.shape
    vsize = 128
    width = pieces[0].shape[2] - vsize
    place_count = sum(piece.shape[0] for piece in pieces)
    rows = SPAN * chunk
    q_row = 0 if number else 2
    lanes_out = 2 * vsize * (number + 1) + vsize
    scalar = pl.BlockSpec(memory_space=pltpu.SMEM)

    def own_block(b, meta):
        return ((meta[1] + b) % blocks, 0, 0)

    specs = [scalar, scalar, pl.BlockSpec((1, width, chunk), lambda b, meta: (b, q_row, 0))]
    specs += [pl.BlockSpec(piece.shape, lambda b, meta: (0, 0, 0)) for piece in pieces]
    operands = [slope, lam, queries, *pieces]
    if number:
        specs.append(pl.BlockSpec((1, chunk, prior.shape[2]), own_block))
        operands.append(prior)
    return pl.pallas_call(
        lambda *refs: flash_body(*refs, first_axis=first_axis, number=number),
        grid_spec=pltpu.PrefetchScalarGridSpec(
            num_scalar_prefetch=1,
            grid=(blocks,),
            in_specs=specs,
            out_specs=pl.BlockSpec((1, chunk, lanes_out), own_block),
            scratch_shapes=[
                pltpu.VMEM((place_count, chunk, width), jnp.bfloat16),
                pltpu.VMEM((place_count, vsize, chunk), jnp.bfloat16),
                pltpu.VMEM((width, 2 * chunk), jnp.bfloat16),
                pltpu.VMEM((rows, LANES), jnp.float32),
                pltpu.VMEM((1, 2 * chunk), jnp.float32),
                pltpu.VMEM((vsize + 16, 2 * chunk), jnp.float32),
                pltpu.VMEM((2, rows, 2 * chunk), jnp.float32),
                pltpu.VMEM((2, 1, 2 * chunk), jnp.float32),
                pltpu.VMEM((vsize, chunk), jnp.float32),
            ],
        ),
        out_shape=jax.ShapeDtypeStruct((blocks, chunk, lanes_out), jnp.bfloat16),
        cost_estimate=pl.CostEstimate(flops=20_000_000_000, transcendentals=0, bytes_accessed=0),
        compiler_params=pltpu.CompilerParams(
            dimension_semantics=("arbitrary",), vmem_limit_bytes=VMEM_LIMIT
        ),
    )(meta, *operands)


def neighbours(size):
    ahead = [((i + 1) % size, i) for i in range(size)]
    behind = [((i - 1) % size, i) for i in range(size)]
    return ahead, behind


def passed_on(value, one, three, axis):
    ahead, behind = neighbours(lax.axis_size(axis))
    cut = value.shape[0] // 2
    two_first = lax.ppermute(one[:cut], axis, ahead)
    two_last = lax.ppermute(three[cut:], axis, behind)
    return [value, one, two_first, two_last, three]


def first_sends(value, axis):
    ahead, behind = neighbours(lax.axis_size(axis))
    return value, lax.ppermute(value, axis, ahead), lax.ppermute(value, axis, behind)


def mirrored_sends(value, axis):
    planes, size = lax.axis_size("z"), lax.axis_size(axis)

    def send(step):
        pairs = [
            ((planes - 1 - z) * size + (i + step) % size, z * size + i)
            for z in range(planes)
            for i in range(size)
        ]
        return lax.ppermute(value, ("z", axis), pairs)

    return send(0), send(1), send(-1)


def stack_body(*refs):
    for outs, pieces in ((refs[10:12], refs[:5]), (refs[12:14], refs[5:10])):
        cut = pieces[2].shape[0]
        outs[0][0] = pieces[0][...]
        outs[0][1] = pieces[1][...]
        outs[1][0, :cut] = pieces[2][...]
        outs[1][0, cut:] = pieces[3][...]
        outs[1][1] = pieces[4][...]


def stacked(first, second):
    shapes = [jax.ShapeDtypeStruct((2, *pieces[0].shape), jnp.bfloat16) for pieces in (first, second)]
    return pl.pallas_call(
        stack_body,
        in_specs=[pl.BlockSpec(memory_space=pltpu.VMEM)] * 10,
        out_shape=[shapes[0], shapes[0], shapes[1], shapes[1]],
        compiler_params=pltpu.CompilerParams(vmem_limit_bytes=VMEM_LIMIT),
    )(*first, *second)


def around_in_halves(front, back, axis):
    ahead, behind = neighbours(lax.axis_size(axis))
    one_front = lax.ppermute(front, axis, ahead)
    three_back = lax.ppermute(back, axis, behind)
    one_back = lax.ppermute(back, axis, ahead)
    three_front = lax.ppermute(front, axis, behind)
    two_front = lax.ppermute(one_front, axis, ahead)
    two_back = lax.ppermute(three_back, axis, behind)
    return [front, back, one_front, one_back, two_front, two_back, three_front, three_back]


def normed(values, gain_row):
    average = jnp.mean(values, axis=-1, keepdims=True)
    centred = values - average
    variance = jnp.mean(centred * centred, axis=-1, keepdims=True)
    return centred * lax.rsqrt(variance + epsilon) * gain_row


def merge_body(core, arrived, head_gain, residual, weight, norm_gain, middle, keep, give):
    planes = arrived.shape[0] // 2
    vsize = head_gain.shape[1]
    gain = head_gain[...].astype(jnp.float32)
    pieces = []
    for head in range(2):
        tails = []
        for z in range(planes):
            lanes = arrived[2 * z + head, :, 4 * vsize :].astype(jnp.float32)
            tails.append([lanes[:, i : i + 1] + lanes[:, i + 6 : i + 7] + lanes[:, i + 12 : i + 13] for i in range(6)])
        for group in range(2):
            mixtures = []
            for j in range(2):
                index = 2 * group + j
                highest = tails[0][index]
                for z in range(1, planes):
                    highest = jnp.maximum(highest, tails[z][index])
                weights = [jnp.exp2(tails[z][index] - highest) for z in range(planes)]
                scaled = 1.0 / sum(weights)
                column = index * vsize
                mixtures.append(
                    sum(
                        (weights[z] * scaled)
                        * arrived[2 * z + head, :, column : column + vsize].astype(jnp.float32)
                        for z in range(planes)
                    )
                )
            head_out = mixtures[0] - tails[0][4 + group] * mixtures[1]
            power = jnp.mean(head_out * head_out, axis=-1, keepdims=True)
            pieces.append((head_out * lax.rsqrt(power + epsilon) * gain).astype(jnp.bfloat16))
    attended = jnp.concatenate(pieces, axis=1)
    projected = jnp.dot(attended, weight[...], preferred_element_type=jnp.float32)
    values = residual_gain * residual[...].astype(jnp.float32) + projected
    result = normed(values, norm_gain[...].astype(jnp.float32)).astype(jnp.bfloat16)
    middle[...] = result
    half = result.shape[1] // 2

    @pl.when(core[0] == 0)
    def _():
        keep[...] = result[:, :half]
        give[...] = result[:, half:]

    @pl.when(core[0] == 1)
    def _():
        keep[...] = result[:, half:]
        give[...] = result[:, :half]


def merge(core, arrived, head_gain, residual, weight, norm_gain):
    count, features = residual.shape
    return pl.pallas_call(
        merge_body,
        in_specs=[pl.BlockSpec(memory_space=pltpu.SMEM)] + [pl.BlockSpec(memory_space=pltpu.VMEM)] * 5,
        out_shape=[
            jax.ShapeDtypeStruct((count, features), jnp.bfloat16),
            jax.ShapeDtypeStruct((count, features // 2), jnp.bfloat16),
            jax.ShapeDtypeStruct((count, features // 2), jnp.bfloat16),
        ],
        cost_estimate=pl.CostEstimate(flops=5_000_000_000, transcendentals=0, bytes_accessed=0),
        compiler_params=pltpu.CompilerParams(vmem_limit_bytes=VMEM_LIMIT),
    )(core, arrived, head_gain, residual, weight, norm_gain)


def expert_body(core, mine, other, gate, up, down, keep, give):
    half = mine.shape[1]
    first = pl.multiple_of(core[0] * half, half)
    second = pl.multiple_of((1 - core[0]) * half, half)
    own_rows = mine[...]
    other_rows = other[...]

    def through(weight):
        return jnp.dot(
            own_rows, weight[0, pl.ds(first, half), :], preferred_element_type=jnp.float32
        ) + jnp.dot(
            other_rows, weight[0, pl.ds(second, half), :], preferred_element_type=jnp.float32
        )

    gate_in = through(gate)
    upward = through(up)
    hidden = (gate_in * (1.0 / (1.0 + jnp.exp(-gate_in))) * upward).astype(jnp.bfloat16)
    keep[...] = jnp.dot(
        hidden, down[0, :, pl.ds(first, half)], preferred_element_type=jnp.float32
    ).astype(jnp.bfloat16)
    give[...] = jnp.dot(
        hidden, down[0, :, pl.ds(second, half)], preferred_element_type=jnp.float32
    ).astype(jnp.bfloat16)


def expert(core, mine, other, gate, up, down):
    count, half = mine.shape
    block_rows = 256
    rows = pl.BlockSpec((block_rows, half), lambda i: (i, 0))
    shape = jax.ShapeDtypeStruct((count, half), jnp.bfloat16)
    return pl.pallas_call(
        expert_body,
        grid=(count // block_rows,),
        in_specs=[
            pl.BlockSpec(memory_space=pltpu.SMEM),
            rows,
            rows,
            pl.BlockSpec(gate.shape, lambda i: (0, 0, 0)),
            pl.BlockSpec(up.shape, lambda i: (0, 0, 0)),
            pl.BlockSpec(down.shape, lambda i: (0, 0, 0)),
        ],
        out_specs=[rows, rows],
        out_shape=[shape, shape],
        cost_estimate=pl.CostEstimate(flops=count * 12_000_000, transcendentals=0, bytes_accessed=0),
        compiler_params=pltpu.CompilerParams(
            dimension_semantics=("arbitrary",), vmem_limit_bytes=VMEM_LIMIT
        ),
    )(core, mine, other, gate, up, down)


def final_body(core, own, received, middle, norm_gain, out, total):
    half = own.shape[1]

    @pl.when(core[0] == 0)
    def _():
        total[:, :half] = own[...]
        total[:, half:] = received[...]

    @pl.when(core[0] == 1)
    def _():
        total[:, :half] = received[...]
        total[:, half:] = own[...]

    values = residual_gain * middle[...].astype(jnp.float32) + total[...]
    out[...] = normed(values, norm_gain[...].astype(jnp.float32)).astype(jnp.bfloat16)


def final(core, own, received, middle, norm_gain):
    return pl.pallas_call(
        final_body,
        in_specs=[pl.BlockSpec(memory_space=pltpu.SMEM)] + [pl.BlockSpec(memory_space=pltpu.VMEM)] * 4,
        out_shape=jax.ShapeDtypeStruct(middle.shape, jnp.bfloat16),
        scratch_shapes=[pltpu.VMEM(middle.shape, jnp.float32)],
        cost_estimate=pl.CostEstimate(flops=2_000_000_000, transcendentals=0, bytes_accessed=0),
        compiler_params=pltpu.CompilerParams(vmem_limit_bytes=VMEM_LIMIT),
    )(core, own, received, middle, norm_gain)


def slots(routes, experts, offset):
    chosen = routes.reshape(-1)
    matches = (chosen[:, None] == jnp.arange(experts)[None, :]).astype(jnp.int32)
    earlier = jnp.cumsum(matches, axis=0) - matches
    rank = jnp.sum(earlier * matches, axis=1)
    return routes, (offset + rank).reshape(routes.shape)


def shards(
    query_small,
    key_small,
    value_small,
    query_large,
    key_large,
    value_large,
    lambdas,
    slopes,
    head_gain,
    residual,
    out_weight,
    norm_gains,
    routes,
    route_weights,
    gate_weight,
    up_weight,
    down_weight,
):
    length = query_small.shape[0]
    planes = lax.axis_size("z")
    plane = lax.axis_index("z")
    core = lax.axis_index("tp")
    swap = [(0, 1), (1, 0)]
    small_pack = jnp.concatenate(
        [key_small.reshape(length, -1), value_small.reshape(length, -1)], axis=1
    )
    large_pack = jnp.concatenate(
        [key_large.reshape(length, -1), value_large.reshape(length, -1)], axis=1
    )
    query_pack = jnp.concatenate(
        [query_large.reshape(length, -1).T, query_small.reshape(length, -1).T], axis=0
    )
    large_parts = passed_on(*first_sends(large_pack, "x"), "x")
    small_parts = passed_on(*mirrored_sends(small_pack, "y"), "y")
    rows = stacked(large_parts, small_parts)
    rows, query_pack = lax.optimization_barrier((rows, query_pack))
    query_sends = first_sends(query_pack, "z")
    large_pieces = around_in_halves(rows[0], rows[1], "y")
    small_pieces = around_in_halves(rows[2], rows[3], "x")
    queries = jnp.concatenate(passed_on(*query_sends, "z"), axis=0)
    queries = queries.reshape(planes, *query_pack.shape)

    core_count = lax.axis_size("tp")
    row_count = length // core_count
    experts = lax.axis_size(SP)
    block = core_count * (4 * row_count // experts)
    their_routes = lax.ppermute(routes, "tp", swap)
    their_weights = lax.ppermute(route_weights, "tp", swap)
    capacity = block // core_count
    tickets = [
        slots(routes, experts, core * capacity),
        slots(their_routes, experts, (1 - core) * capacity),
    ]
    chosen = jnp.concatenate([tickets[0][0], tickets[1][0]], axis=0)
    spot = jnp.concatenate([tickets[0][1], tickets[1][1]], axis=0)
    shares = jnp.concatenate([route_weights, their_weights], axis=0)
    cuts = ((0, 16), (16, 8))
    selectors = []
    spreads = []
    for first, width in cuts:
        row = jnp.where((spot >= first) & (spot < first + width), chosen * width + spot - first, -1)
        places = jnp.arange(experts * width)
        selectors.append(
            ((row[:, 0][None, :] == places[:, None]) | (row[:, 1][None, :] == places[:, None])).astype(
                jnp.bfloat16
            )
        )
        spread = jnp.where(row[:, 0][:, None] == places[None, :], shares[:, :1], 0.0) + jnp.where(
            row[:, 1][:, None] == places[None, :], shares[:, 1:], 0.0
        )
        spread_top = lax.reduce_precision(spread, exponent_bits=8, mantissa_bits=7)
        spreads.append((spread_top.astype(jnp.bfloat16), (spread - spread_top).astype(jnp.bfloat16)))

    home = [plane, lax.axis_index("y"), lax.axis_index("x")]
    small_meta = jnp.stack([planes - 1 - plane, *home]).astype(jnp.int32)
    large_meta = jnp.stack([plane, *home]).astype(jnp.int32)
    parts = flash(
        0, small_meta, slopes[0, :1], lambdas[0, :1], queries, small_pieces, None, "y"
    )
    parts = flash(
        1, large_meta, slopes[0, 1:], lambdas[0, 1:], queries, large_pieces, parts, "x"
    )
    parts = parts.reshape(planes * core_count, row_count, -1)
    parts = lax.all_to_all(parts, OWNERS, split_axis=0, concat_axis=0, tiled=True)
    which = core.astype(jnp.int32).reshape(1)
    middle, keep, give = merge(
        which, parts, head_gain.reshape(1, -1), residual, out_weight, norm_gains[:1]
    )
    half = keep.shape[1]
    tokens = jnp.concatenate([keep, lax.ppermute(give, "tp", swap)], axis=0)
    arrived = []
    for (first, width), selector in zip(cuts, selectors):
        outgoing = jnp.dot(selector, tokens, preferred_element_type=jnp.float32).astype(jnp.bfloat16)
        came = lax.all_to_all(
            outgoing.reshape(experts, width, half), SP, split_axis=0, concat_axis=0, tiled=True
        )
        arrived.append(came.reshape(experts * width, half))
    returned = []
    for (first, width), mine in zip(cuts, arrived):
        other = lax.ppermute(mine, "tp", swap)
        kept, given = expert(which, mine, other, gate_weight, up_weight, down_weight)
        got = lax.ppermute(given, "tp", swap)
        summed = (kept.astype(jnp.float32) + got.astype(jnp.float32)).astype(jnp.bfloat16)
        came = lax.all_to_all(
            summed.reshape(experts, width, half), SP, split_axis=0, concat_axis=0, tiled=True
        )
        returned.append(came.reshape(experts * width, half))

    def weighed(first):
        cut = slice(first, first + row_count)
        return sum(
            jnp.dot(high[cut], rows, preferred_element_type=jnp.float32)
            + jnp.dot(low[cut], rows, preferred_element_type=jnp.float32)
            for (high, low), rows in zip(spreads, returned)
        )

    received = lax.ppermute(weighed(row_count), "tp", swap)
    return final(which, weighed(0), received, middle, norm_gains[1:])


def solution(mesh):
    cube = Mesh(mesh.devices.reshape(4, 4, 4, 2), ("z", "y", "x", "tp"))
    both = SP + ("tp",)
    placed = (
        P(SP, "tp", None),
        P(SP, "tp", None),
        P(SP, "tp", None),
        P(SP, "tp", None),
        P(SP, "tp", None),
        P(SP, "tp", None),
        P("tp", None),
        P("tp", None),
        P(),
        P(both, None),
        P(),
        P(),
        P(both, None),
        P(both, None),
        P(SP, None, "tp"),
        P(SP, None, "tp"),
        P(SP, "tp", None),
    )

    return jax.shard_map(
        shards, mesh=cube, in_specs=placed, out_specs=P(both, None), check_vma=False
    )
```
